32 devices in a mesh: sp: 4 (over z), fs: 4 (over y, x), tp: 2 (over core).
Axes of the slice: x: 2, y: 2, z: 4, core: 2. Of those that a mesh axis runs over, the one named last changes fastest.
Arguments:
- inputs: bfloat16 [4, 512, 2048], P('fs', 'sp'), may hold values from -6 to 6
- input_norm_gain: bfloat16 [2048], replicated, may hold values from 0.099609375 to 1.8984375
- receptance_matrix: bfloat16 [2048, 1024], P('fs', 'tp'), may hold values from -0.125 to 0.125
- key_matrix: bfloat16 [2048, 1024], P('fs', 'tp'), may hold values from -0.125 to 0.125
- value_matrix: bfloat16 [2048, 1024], P('fs', 'tp'), may hold values from -0.125 to 0.125
- pooling_input_weight: bfloat16 [2048, 1024], P('fs', 'tp'), may hold values from -0.125 to 0.125
- decay_lower_matrix: bfloat16 [2048, 128], replicated, may hold values from -0.125 to 0.125
- decay_raise_matrix: bfloat16 [2, 64, 1024], P(None, None, 'tp'), may hold values from -1 to 1
- decay_offset_bias: float32 [2, 1024], P(None, 'tp'), may hold values from -13 to -3
- removal_lower_matrix: bfloat16 [2048, 128], replicated, may hold values from -0.125 to 0.125
- removal_raise_matrix: bfloat16 [2, 64, 1024], P(None, None, 'tp'), may hold values from -1 to 1
- removal_rate_bias: float32 [2, 1024], P(None, 'tp'), may hold values from -9 to 1.5
- tempo_scale: float32 [4, 2, 16, 512], P('fs', None, 'tp', 'sp'), may hold values from 0.3 to 3.2, as said below
- sudden_decay_extra: float32 [4, 2, 16, 512], P('fs', None, 'tp', 'sp'), may hold values from -2.8 to 0
- head_norm_gain: bfloat16 [1024], P('tp'), may hold values from 0.099609375 to 1.8984375
- group_mixing_weight: bfloat16 [4, 256, 256], P('tp'), may hold values from -0.375 to 0.375
- attention_output_matrix: bfloat16 [2048, 1024], P('fs', 'tp'), may hold values from -0.125 to 0.125
- pooling_output_matrix: bfloat16 [2048, 1024], P('fs', 'tp'), may hold values from -0.125 to 0.125
Outputs:
- mixed_out: bfloat16 [4, 512, 2048], P('fs', ('sp', 'tp'))
The draws below stay inside these ranges and needn't reach their ends.
Inputs may be any that keep to these rules, and one draw needn't show every extreme that they name: `tempo_scale`: positive.
All inputs are finite; a program needn't handle non-finite values.
Results may differ from the reference program's by a relative error of at most 0.017.
Values may be sent and summed in bfloat16 or wider, within the bound.
A program may use at most 128 MiB of HBM per device.

```python
import math
import jax
import jax.numpy as jnp
from jax import lax

D = 2048
HEADS_A = 16
HEAD = 64
DECAY_RANK = 64
RATE_RANK = 64
POOL_GROUPS = 4
GROUP_WIDTH = 256
T_DEV = 128
D_A = 1024
D_POOL = 1024
LEN = 512
SEQS = 4
N_SP = 4


def slow_mask(key):
    marks = []
    for travel_direction in range(2):
        order = jax.random.permutation(jax.random.fold_in(key, 41 + travel_direction), HEADS_A)
        marks.append((order < HEADS_A // 2).astype(jnp.float32))
    return jnp.repeat(jnp.stack(marks, axis=0), HEAD, axis=1)


def draw_decay_offset_bias(key, part):
    slow = slow_mask(key)
    jitter = jax.random.uniform(jax.random.fold_in(key, 5), (2, HEADS_A * HEAD), jnp.float32, -0.5, 0.5)
    slow_level = jnp.log(1.0 / (6.0 * LEN)) + 0.1
    fast_level = math.log(1.0 / 60.0) + 0.5
    return slow * slow_level + (1.0 - slow) * fast_level + jitter


def draw_removal_rate_bias(key, part):
    slow = slow_mask(key)
    jitter = jax.random.uniform(jax.random.fold_in(key, 6), (2, HEADS_A * HEAD), jnp.float32, -0.5, 0.5)
    fast_vals = jax.random.uniform(jax.random.fold_in(key, 7), (2, HEADS_A * HEAD), jnp.float32, -1.5, 1.5)
    return slow * (jnp.log(8.0 / LEN) + jitter) + (1.0 - slow) * fast_vals


def draw_tempo_scale(key, part):
    low, high = (0.5, 2.0)
    factor = jnp.exp(jax.random.uniform(jax.random.fold_in(key, 21), (SEQS, 2, HEADS_A, N_SP), jnp.float32, math.log(low), math.log(high)))
    factor = jnp.repeat(factor, T_DEV, axis=3)
    jitter = jax.random.uniform(jax.random.fold_in(key, 22), (SEQS, 2, HEADS_A, LEN), jnp.float32, 0.8, 1.25)
    return factor * jitter


def draw_sudden_decay_extra(key, part):
    places = jax.random.randint(jax.random.fold_in(key, 31), (SEQS, 2, HEADS_A, 4), 0, LEN)
    kept = jax.random.uniform(jax.random.fold_in(key, 32), (SEQS, 2, HEADS_A, 4), jnp.float32, 0.5, 0.8)
    lost = jnp.log(kept)
    spots = jnp.arange(LEN)
    marked = jnp.where(spots[None, None, None, None, :] == places[..., None], lost[..., None], 0.0)
    return jnp.sum(marked, axis=3).astype(jnp.float32)


def levels(stream_key, shape, shards, smallest, high):
    def one(axis_at, blocks):
        heights = jax.random.uniform(jax.random.fold_in(jax.random.fold_in(stream_key, 6), axis_at), (blocks,), jnp.float32, smallest / len(shards), high / len(shards))
        return jnp.repeat(jnp.exp(heights), shape[axis_at] // blocks).reshape((-1,) + (1,) * (len(shape) - axis_at - 1))

    factor_of = one(*shards[0])
    for cut in shards[1:]:
        factor_of = factor_of * one(*cut)
    return factor_of


def scatter_about(key, shape, deviation, most, pieces=(), dtype=jnp.bfloat16):
    drawn = deviation * jax.random.normal(key, shape, jnp.float32)
    if pieces:
        drawn = drawn * levels(key, shape, pieces, -0.22, 0.18)
    return jnp.clip(drawn, -most, most).astype(dtype)


def setup_inputs(seed: int = 0) -> dict:
    keys = jax.random.split(jax.random.key(seed), 19)
    inputs = scatter_about(keys[0], (SEQS, LEN, D), 1.0, 6.0, ((0, 4), (1, 4)))
    input_norm_gain = jnp.clip(1.0 + 0.18 * jax.random.normal(keys[1], (D,), jnp.float32), 0.099609375, 1.8984375).astype(jnp.bfloat16)
    receptance_matrix = scatter_about(keys[2], (D, D_A), D ** -0.5, 0.125, ((0, 4), (1, 2)))
    key_matrix = scatter_about(keys[3], (D, D_A), D ** -0.5, 0.125, ((0, 4), (1, 2)))
    value_matrix = scatter_about(keys[4], (D, D_A), D ** -0.5, 0.125, ((0, 4), (1, 2)))
    pooling_input_weight = scatter_about(keys[5], (D, D_POOL), D ** -0.5, 0.125, ((0, 4), (1, 2)))
    decay_lower_matrix = scatter_about(keys[6], (D, 2 * DECAY_RANK), D ** -0.5, 0.125)
    decay_raise_matrix = scatter_about(keys[7], (2, DECAY_RANK, D_A), (DECAY_RANK // 2) ** -0.5, 1.0, ((2, 2),))
    decay_offset_bias = draw_decay_offset_bias(jax.random.fold_in(keys[18], 71), 0)
    removal_lower_matrix = scatter_about(keys[9], (D, 2 * RATE_RANK), D ** -0.5, 0.125)
    removal_raise_matrix = scatter_about(keys[10], (2, RATE_RANK, D_A), (RATE_RANK // 2) ** -0.5, 1.0, ((2, 2),))
    removal_rate_bias = draw_removal_rate_bias(jax.random.fold_in(keys[18], 71), 0)
    tempo_scale = draw_tempo_scale(jax.random.fold_in(keys[18], 71), 0)
    sudden_decay_extra = draw_sudden_decay_extra(jax.random.fold_in(keys[18], 71), 0)
    head_norm_gain = jnp.clip(1.0 + 0.18 * jax.random.normal(keys[14], (D_A,), jnp.float32), 0.099609375, 1.8984375).astype(jnp.bfloat16)
    group_mixing_weight = scatter_about(keys[15], (POOL_GROUPS, GROUP_WIDTH, GROUP_WIDTH), GROUP_WIDTH ** -0.5, 0.375, ((0, 2),))
    attention_output_matrix = scatter_about(keys[16], (D, D_A), (D_A + D_POOL) ** -0.5, 0.125, ((0, 4), (1, 2)))
    pooling_output_matrix = scatter_about(keys[17], (D, D_POOL), (D_A + D_POOL) ** -0.5, 0.125, ((0, 4), (1, 2)))
    return dict(inputs=inputs, input_norm_gain=input_norm_gain, receptance_matrix=receptance_matrix, key_matrix=key_matrix, value_matrix=value_matrix, pooling_input_weight=pooling_input_weight, decay_lower_matrix=decay_lower_matrix, decay_raise_matrix=decay_raise_matrix, decay_offset_bias=decay_offset_bias, removal_lower_matrix=removal_lower_matrix, removal_raise_matrix=removal_raise_matrix, removal_rate_bias=removal_rate_bias, tempo_scale=tempo_scale, sudden_decay_extra=sudden_decay_extra, head_norm_gain=head_norm_gain, group_mixing_weight=group_mixing_weight, attention_output_matrix=attention_output_matrix, pooling_output_matrix=pooling_output_matrix)


norm_eps = 1e-06
head_eps = 0.00064
unit_eps = 1e-06
highest = lax.Precision.HIGHEST

def project(left, weight):
    return jnp.dot(left, weight, preferred_element_type=jnp.float32).astype(jnp.bfloat16)

def window_diff(values, half):
    running = jnp.concatenate([jnp.zeros((1, values.shape[1]), jnp.float32), jnp.cumsum(values, axis=0)], axis=0)
    spots = jnp.arange(LEN)
    upper = jnp.minimum(spots + half, LEN)
    lower = jnp.maximum(spots - half, 0)
    counts = (upper - lower).astype(jnp.float32)
    return (running[upper] - running[lower]) / counts[:, None] - values

def recur(state, element_list):
    decay, unit, removal, written, value, recept = element_list
    pulled = jnp.einsum('hvk,hk->hv', state, unit, precision=highest)
    state = state * jnp.exp(decay)[:, None, :] - pulled[:, :, None] * removal[:, None, :] + value[:, :, None] * written[:, None, :]
    return (state, jnp.einsum('hvk,hk->hv', state, recept, precision=highest))

def reference(inputs, input_norm_gain, receptance_matrix, key_matrix, value_matrix, pooling_input_weight, decay_lower_matrix, decay_raise_matrix, decay_offset_bias, removal_lower_matrix, removal_raise_matrix, removal_rate_bias, tempo_scale, sudden_decay_extra, head_norm_gain, group_mixing_weight, attention_output_matrix, pooling_output_matrix):

    def single_sequence(element_list):
        row_block, decay_tempo, sudden_jump = element_list
        values = row_block.astype(jnp.float32)
        normed = (values * lax.rsqrt(lax.optimization_barrier(jnp.mean(values * values, axis=-1, keepdims=True)) + norm_eps) * input_norm_gain.astype(jnp.float32)).astype(jnp.bfloat16)
        receptance = project(normed, receptance_matrix).astype(jnp.float32).reshape(LEN, HEADS_A, HEAD)
        key_rows = project(normed, key_matrix).astype(jnp.float32).reshape(LEN, HEADS_A, HEAD)
        val_rows = project(normed, value_matrix).astype(jnp.float32).reshape(LEN, HEADS_A, HEAD)
        pool_in = project(normed, pooling_input_weight).astype(jnp.float32)
        decay_act = jnp.tanh(project(normed, decay_lower_matrix).astype(jnp.float32)).astype(jnp.bfloat16)
        rate_latent = project(normed, removal_lower_matrix)
        unit_keys = key_rows * lax.rsqrt(lax.optimization_barrier(jnp.sum(key_rows * key_rows, axis=-1, keepdims=True)) + unit_eps)
        readout = jnp.zeros((LEN, HEADS_A, HEAD), jnp.float32)
        for travel_direction in range(2):
            part = decay_act[:, travel_direction * DECAY_RANK:(travel_direction + 1) * DECAY_RANK]
            decay_pre = decay_offset_bias[travel_direction] + jnp.dot(part, decay_raise_matrix[travel_direction], preferred_element_type=jnp.float32)
            decay_velocity = jnp.exp(-jax.nn.softplus(-decay_pre) - 0.5).reshape(LEN, HEADS_A, HEAD)
            logarithm_decay = -decay_velocity * decay_tempo[travel_direction].T[:, :, None] + sudden_jump[travel_direction].T[:, :, None]
            latent = rate_latent[:, travel_direction * RATE_RANK:(travel_direction + 1) * RATE_RANK]
            rate = jax.nn.sigmoid(removal_rate_bias[travel_direction] + jnp.dot(latent, removal_raise_matrix[travel_direction], preferred_element_type=jnp.float32))
            rate = rate.reshape(LEN, HEADS_A, HEAD)
            start = jnp.zeros((HEADS_A, HEAD, HEAD), jnp.float32)
            _, reads = lax.scan(recur, start, (logarithm_decay, unit_keys, unit_keys * rate, key_rows * rate, val_rows, receptance), reverse=travel_direction == 1)
            readout = readout + reads
        centred = readout - lax.optimization_barrier(jnp.mean(readout, axis=-1, keepdims=True))
        spread = lax.optimization_barrier(jnp.mean(centred * centred, axis=-1, keepdims=True))
        attn_out = (centred * lax.rsqrt(spread + head_eps)).reshape(LEN, HEADS_A * HEAD) * head_norm_gain.astype(jnp.float32)
        attn_out = attn_out.astype(jnp.bfloat16)
        diffs = [window_diff(pool_in[:, group * GROUP_WIDTH:(group + 1) * GROUP_WIDTH], 2 ** group) for group in range(POOL_GROUPS)]
        pool_diff = jnp.concatenate(diffs, axis=1).astype(jnp.bfloat16)
        mixed = [jnp.dot(pool_diff[:, group * GROUP_WIDTH:(group + 1) * GROUP_WIDTH], group_mixing_weight[group], preferred_element_type=jnp.float32) for group in range(POOL_GROUPS)]
        pool_out = jnp.concatenate(mixed, axis=1).astype(jnp.bfloat16)
        merged = jnp.dot(attn_out, attention_output_matrix.T, preferred_element_type=jnp.float32) + jnp.dot(pool_out, pooling_output_matrix.T, preferred_element_type=jnp.float32)
        return merged.astype(jnp.bfloat16)
    return lax.map(single_sequence, (inputs, tempo_scale, sudden_decay_extra))
```

```python
import functools

import jax
import jax.numpy as jnp
from jax import lax
from jax.experimental import pallas as pl
from jax.experimental.pallas import tpu as pltpu
from jax.sharding import PartitionSpec as P

HEAD = 64
GROUP_WIDTH = 256
LANES = 128
BLOCK = 16
HALO = 16

norm_eps = 1e-06
head_eps = 0.00064
unit_eps = 1e-06
f32 = jnp.float32
bf16 = jnp.bfloat16
VMEM = pl.BlockSpec(memory_space=pltpu.VMEM)


def dot(left, right):
    return jnp.dot(left.astype(bf16), right.astype(bf16), preferred_element_type=f32)


def dot_general(left, right, dims):
    return lax.dot_general(
        left.astype(bf16), right.astype(bf16), (dims, ((), ())), preferred_element_type=f32
    )


def dot_rows(left, right):
    return dot_general(left, right, ((1,), (1,)))


def dot_cols(left, right):
    return dot_general(left, right, ((0,), (0,)))


def exact_dot(left, right, dims):
    return lax.dot_general(
        left, right, (dims, ((), ())), preferred_element_type=f32, precision=lax.Precision.HIGHEST
    )


def remote(src, dst, send, recv, axis, peer):
    return pltpu.make_async_remote_copy(
        src_ref=src,
        dst_ref=dst,
        send_sem=send,
        recv_sem=recv,
        device_id={axis: peer},
        device_id_type=pl.DeviceIdType.MESH,
    )


def greet(barrier, axis, peer):
    pl.semaphore_signal(
        barrier, inc=1, device_id={axis: peer}, device_id_type=pl.DeviceIdType.MESH
    )


def front_kernel(
    n,
    x_ref,
    gain_ref,
    wr_ref,
    wk_ref,
    wv_ref,
    wp_ref,
    dl_ref,
    rl_ref,
    out_ref,
    lat_ref,
    mine,
    cells,
    part,
    landed,
    xs,
    xr,
    ps,
    pr,
):
    me = lax.axis_index("fs")
    barrier = pltpu.get_barrier_semaphore()
    for d in range(1, n):
        greet(barrier, "fs", lax.rem(me + d, n))
    width = wr_ref.shape[0]
    x = x_ref[0].astype(f32)
    normed = (
        x
        * lax.rsqrt(jnp.mean(x * x, axis=-1, keepdims=True) + norm_eps)
        * gain_ref[...].astype(f32)
    ).astype(bf16)
    for j in range(n):
        mine[j] = normed[:, j * width : (j + 1) * width]
    pl.semaphore_wait(barrier, n - 1)
    order = [n // 2] + [d for d in range(1, n) if d != n // 2]
    moves = []
    for d in order:
        peer = lax.rem(me + d, n)
        copy = remote(mine.at[peer], cells.at[me], xs.at[d], xr.at[d], "fs", peer)
        copy.start()
        moves.append(copy)
    decay = jnp.zeros((x.shape[0], dl_ref.shape[1]), f32)
    rate = jnp.zeros((x.shape[0], rl_ref.shape[1]), f32)
    for j in range(n):
        block = mine[j]
        decay = decay + dot(block, dl_ref[j * width : (j + 1) * width])
        rate = rate + dot(block, rl_ref[j * width : (j + 1) * width])
    lat_ref[0] = jnp.tanh(decay.astype(bf16).astype(f32)).astype(bf16)
    lat_ref[1] = rate.astype(bf16)
    weights = (wk_ref, wr_ref, wv_ref, wp_ref)
    copies = []
    for copy, d in zip(moves, order):
        copy.wait_recv()
    for m, weight in enumerate(weights):
        for d in order:
            peer = lax.rem(me + d, n)
            part[peer, m] = dot(cells[peer], weight[...]).astype(bf16)
            copy = remote(
                part.at[peer, m], landed.at[me, m], ps.at[d, m], pr.at[d, m], "fs", peer
            )
            copy.start()
            copies.append((m, copy))
    for m, weight in enumerate(weights):
        total = dot(mine[me], weight[...])
        for at, copy in copies:
            if at == m:
                copy.wait_recv()
        for d in range(1, n):
            total = total + landed[lax.rem(me + d, n), m].astype(f32)
        out_ref[m] = total.astype(bf16)
    for copy in moves:
        copy.wait_send()
    for _, copy in copies:
        copy.wait_send()


def mixer_kernel(
    p4_ref,
    lat_ref,
    draise_ref,
    dbias_ref,
    rraise_ref,
    rbias_ref,
    tempo_ref,
    extra_ref,
    query_ref,
    local_ref,
    transfer_ref,
    carried_ref,
):
    pair = pl.program_id(0)
    tokens = p4_ref.shape[1]
    kf = p4_ref[0].astype(f32)
    rf = p4_ref[1].astype(f32)
    value = p4_ref[2]
    lane = lax.broadcasted_iota(jnp.int32, (tokens, LANES), 1)
    row = lax.broadcasted_iota(jnp.int32, (tokens, LANES), 0)
    head0 = lane < HEAD
    k2 = kf * kf
    s0 = jnp.sum(jnp.where(head0, k2, 0.0), axis=-1, keepdims=True)
    s1 = jnp.sum(jnp.where(head0, 0.0, k2), axis=-1, keepdims=True)
    unit = kf * lax.rsqrt(jnp.where(head0, s0, s1) + unit_eps)
    heads = tempo_ref.shape[1]
    spread = (
        lax.broadcasted_iota(jnp.int32, (heads, LANES), 0)
        == 2 * pair + lax.broadcasted_iota(jnp.int32, (heads, LANES), 1) // HEAD
    ).astype(f32)
    blocks = tokens // BLOCK
    zero_row = jnp.zeros((1, LANES), f32)
    eye = (row == lane).astype(f32)
    sizes = []
    size = 1
    while size < tokens:
        sizes.append(size)
        size *= 2

    def level_mask(k):
        return ((row >> (k + 1)) == (lane >> (k + 1))) & ((row >> k) != (lane >> k))

    ways = []
    for d in range(2):
        lat_mask = head0 if d == 0 else ~head0
        lat_d = jnp.where(lat_mask, lat_ref[0].astype(f32), 0.0)
        lat_r = jnp.where(lat_mask, lat_ref[1].astype(f32), 0.0)
        pre = dbias_ref[d : d + 1] + dot(lat_d, draise_ref[...])
        velocity = jax.nn.sigmoid(pre) * 0.6065306597126334
        tempo = exact_dot(tempo_ref[d], spread, ((0,), (0,)))
        extra = exact_dot(extra_ref[d], spread, ((0,), (0,)))
        ld = -velocity * tempo + extra
        rate = jax.nn.sigmoid(rbias_ref[d : d + 1] + dot(lat_r, rraise_ref[...]))
        removal = unit * rate
        written = kf * rate
        upto = (lane <= row) if d == 0 else (lane >= row)
        inner = exact_dot(upto.astype(f32), ld, ((1,), (0,)))
        excl = inner - ld
        grams = []
        for i in range(blocks):
            lo, hi = i * BLOCK, (i + 1) * BLOCK
            if d == 0:
                base = inner[lo - 1 : lo] if i > 0 else zero_row
            else:
                base = inner[hi : hi + 1] if i < blocks - 1 else zero_row
            ahead = unit[lo:hi] * jnp.exp(excl[lo:hi] - base)
            query = rf[lo:hi] * jnp.exp(inner[lo:hi] - base)
            grow = jnp.exp(jnp.minimum(base - inner, 80.0))
            right = jnp.concatenate([(removal * grow).astype(bf16), (written * grow).astype(bf16)], 0)
            h0 = head0[lo:hi]
            left = jnp.concatenate(
                [
                    jnp.where(h0, ahead, 0.0),
                    jnp.where(h0, 0.0, ahead),
                    jnp.where(h0, query, 0.0),
                    jnp.where(h0, 0.0, query),
                ],
                0,
            )
            grams.append(dot_rows(left, right))
        strict = (lane < row) if d == 0 else (lane > row)

        def gathered(place, at, mask):
            rows = jnp.concatenate(
                [g[place * BLOCK : (place + 1) * BLOCK, at * tokens : (at + 1) * tokens] for g in grams],
                0,
            )
            return jnp.where(mask, rows, 0.0)

        way = dict(inner=inner, excl=excl, removal=removal, written=written)
        way["link"] = [gathered(h, 0, strict) for h in range(2)]
        way["link_write"] = [gathered(h, 1, strict).astype(bf16) for h in range(2)]
        way["read"] = [gathered(2 + h, 0, upto).astype(bf16) for h in range(2)]
        way["read_write"] = [gathered(2 + h, 1, upto).astype(bf16) for h in range(2)]
        ways.append(way)

    links = [way["link"][h] for way in ways for h in range(2)]
    inverses = [eye - jnp.where(level_mask(0), a, 0.0) for a in links]
    for k in range(1, len(sizes)):
        mask = level_mask(k)
        firsts = [dot(t, jnp.where(mask, a, 0.0)) for t, a in zip(inverses, links)]
        inverses = [t - dot(u, t) for t, u in zip(inverses, firsts)]

    block_diag = (row < HEAD) == head0
    local = jnp.zeros((tokens, LANES), f32)
    for d, way in enumerate(ways):
        inner, excl = way["inner"], way["excl"]
        last = inner[tokens - 1 : tokens] if d == 0 else inner[0:1]
        ahead = unit * jnp.exp(excl)
        query = rf * jnp.exp(inner)
        tail = jnp.exp(last - inner)

        def chosen(pieces):
            return jnp.where(head0, pieces[0], pieces[1])

        base = chosen([dot(way["link_write"][h], value) for h in range(2)])
        rhs = jnp.concatenate([ahead.astype(bf16), base.astype(bf16)], 1)
        solved = [dot(inverses[2 * d + h], rhs) for h in range(2)]
        pull_map = -chosen([s[:, :LANES] for s in solved])
        pull_base = -chosen([s[:, LANES:] for s in solved])
        remove_tail = (way["removal"] * tail).astype(bf16)
        write_tail = (way["written"] * tail).astype(bf16)
        both = jnp.concatenate([pull_map.astype(bf16), pull_base.astype(bf16)], 1)
        seen = [dot(way["read"][h], both) for h in range(2)]
        query_ref[d] = (query + chosen([s[:, :LANES] for s in seen])).astype(bf16)
        local = (
            local
            + chosen([s[:, LANES:] for s in seen])
            + chosen([dot(way["read_write"][h], value) for h in range(2)])
        )
        transfer = jnp.where(block_diag, dot_cols(pull_map, remove_tail), 0.0) + eye * jnp.exp(last)
        transfer_ref[d, 0] = transfer
        carried = dot_cols(
            jnp.concatenate([pull_base.astype(bf16), value], 0),
            jnp.concatenate([remove_tail, write_tail], 0),
        )
        carried = jnp.where(block_diag, carried, 0.0)
        carried_ref[d, 0] = carried[:HEAD] + carried[HEAD:]
    local_ref[...] = local


def tail_kernel(
    nsp,
    nfs,
    ntp,
    query_ref,
    local_ref,
    transfer_ref,
    carried_ref,
    p4_ref,
    mix_ref,
    gain_ref,
    wa_ref,
    wp_ref,
    out_ref,
    edge,
    halo,
    incoming,
    leaving,
    act,
    tsend,
    trecv,
    osend,
    orecv,
    hs,
    hr,
    ss,
    sr,
    gs,
    gr,
    ts,
    tr,
    os,
    orr,
):
    z = lax.axis_index("sp")
    me = lax.axis_index("fs")
    core = lax.axis_index("tp")
    tokens, channels = local_ref.shape
    pairs = transfer_ref.shape[1]
    half_rows = tokens // ntp
    has_prev = z > 0
    has_next = z < nsp - 1
    prev = jnp.maximum(z - 1, 0)
    after = jnp.minimum(z + 1, nsp - 1)

    barrier = pltpu.get_barrier_semaphore()
    for d in range(1, nfs):
        greet(barrier, "fs", lax.rem(me + d, nfs))
    for d in range(1, ntp):
        greet(barrier, "tp", lax.rem(core + d, ntp))
    pl.when(has_prev)(lambda: greet(barrier, "sp", prev))
    pl.when(has_next)(lambda: greet(barrier, "sp", after))
    count = nfs + ntp - 2 + jnp.where(has_prev, 1, 0) + jnp.where(has_next, 1, 0)
    edge[0] = p4_ref[3, :HALO]
    edge[1] = p4_ref[3, tokens - HALO :]
    pl.semaphore_wait(barrier, count)

    sides = [(has_prev, prev, has_next), (has_next, after, has_prev)]
    state_copies = [
        remote(leaving.at[0], incoming.at[0], ss.at[0], sr.at[0], "sp", after),
        remote(leaving.at[1], incoming.at[1], ss.at[1], sr.at[1], "sp", prev),
    ]
    halo_copies = [
        remote(edge.at[1], halo.at[0], hs.at[0], hr.at[0], "sp", after),
        remote(edge.at[0], halo.at[1], hs.at[1], hr.at[1], "sp", prev),
    ]
    sends = [has_next, has_prev]
    takes = [has_prev, has_next]

    def relay(d):
        @pl.when(takes[d])
        def _():
            state_copies[d].wait_recv()

        @pl.when(jnp.logical_not(takes[d]))
        def _():
            incoming[d] = jnp.zeros_like(incoming[d])

        @pl.when(sends[d])
        def _():
            for p in range(pairs):
                rows = slice(p * HEAD, (p + 1) * HEAD)
                leaving[d, rows] = (
                    dot(incoming[d, rows], transfer_ref[d, p]) + carried_ref[d, p]
                ).astype(bf16)
            state_copies[d].start()

    def start_halo(d):
        pl.when(sends[d])(lambda: halo_copies[d].start())

    early = 2 * z < nsp

    @pl.when(early)
    def _():
        relay(0)

    @pl.when(jnp.logical_not(early))
    def _():
        relay(1)

    for d in range(2):
        start_halo(d)
    for d in range(2):

        @pl.when(takes[d])
        def _():
            halo_copies[d].wait_recv()

        @pl.when(jnp.logical_not(takes[d]))
        def _():
            halo[d] = jnp.zeros_like(halo[d])

    span = tokens + 2 * HALO
    rim = jnp.concatenate([halo[0], p4_ref[3], halo[1]], 0)
    here = lax.broadcasted_iota(jnp.int32, (tokens, span), 0)
    there = lax.broadcasted_iota(jnp.int32, (tokens, span), 1) - HALO
    position = z * tokens + lax.broadcasted_iota(jnp.int32, (tokens, GROUP_WIDTH), 0)
    length = tokens * nsp
    groups_here = channels // GROUP_WIDTH
    for member in range(groups_here):
        cols = slice(member * GROUP_WIDTH, (member + 1) * GROUP_WIDTH)
        reach = jnp.left_shift(1, core * groups_here + member)
        window = jnp.where((there >= here - reach) & (there < here + reach), 1.0, 0.0)
        total = dot(window, rim[:, cols])
        size = (
            jnp.minimum(position + reach, length) - jnp.maximum(position - reach, 0)
        ).astype(f32)
        diff = (total / size - p4_ref[3, :, cols].astype(f32)).astype(bf16)
        act[me, 0, :, cols] = dot(diff, mix_ref[member]).astype(bf16)
    order = [nfs // 2] + [d for d in range(1, nfs) if d != nfs // 2]
    shares = []
    for d in order:
        peer = lax.rem(me + d, nfs)
        copy = remote(act.at[me, 0], act.at[me, 0], gs.at[d, 0], gr.at[d, 0], "fs", peer)
        copy.start()
        shares.append(copy)

    @pl.when(early)
    def _():
        relay(1)

    @pl.when(jnp.logical_not(early))
    def _():
        relay(0)

    head0 = lax.broadcasted_iota(jnp.int32, (tokens, LANES), 1) < HEAD
    top0 = lax.broadcasted_iota(jnp.int32, (HEAD, LANES), 1) < HEAD
    for p in range(pairs):
        lanes = slice(p * LANES, (p + 1) * LANES)
        readout = local_ref[:, lanes]
        for d in range(2):
            state = incoming[d, p * HEAD : (p + 1) * HEAD].astype(f32)
            wide = jnp.concatenate(
                [jnp.where(top0, state, 0.0), jnp.where(top0, 0.0, state)], 0
            )
            readout = readout + dot_rows(query_ref[d, :, lanes], wide)

        def head_mean(cells):
            low = jnp.sum(jnp.where(head0, cells, 0.0), axis=-1, keepdims=True)
            high = jnp.sum(jnp.where(head0, 0.0, cells), axis=-1, keepdims=True)
            return jnp.where(head0, low, high) * (1.0 / HEAD)

        centred = readout - head_mean(readout)
        scaled = centred * lax.rsqrt(head_mean(centred * centred) + head_eps)
        act[me, 1, :, lanes] = (scaled * gain_ref[:, lanes].astype(f32)).astype(bf16)
    for d in order:
        peer = lax.rem(me + d, nfs)
        copy = remote(act.at[me, 1], act.at[me, 1], gs.at[d, 1], gr.at[d, 1], "fs", peer)
        copy.start()
        shares.append(copy)

    other = lax.rem(core + 1, ntp)
    mine_at = pl.multiple_of(core * half_rows, half_rows)
    other_at = pl.multiple_of(other * half_rows, half_rows)

    def product(seq, rows):
        return dot_rows(act[seq, 1, rows], wa_ref[...]) + dot_rows(act[seq, 0, rows], wp_ref[...])

    returns = []
    swaps = []
    turns = [0] + [d for d in range(1, nfs) if d != nfs // 2] + [nfs // 2]
    for d in turns:
        seq = lax.rem(me + nfs - d, nfs)
        if d:
            for copy, at in zip(shares, order + order):
                if at == d:
                    copy.wait_recv()
        tsend[d] = product(seq, pl.ds(other_at, half_rows)).astype(bf16)
        swap = remote(tsend.at[d], trecv.at[d], ts.at[d], tr.at[d], "tp", other)
        swap.start()
        swaps.append(swap)
        kept = product(seq, pl.ds(mine_at, half_rows))
        swap.wait_recv()
        whole = (kept + trecv[d].astype(f32)).astype(bf16)
        if d:
            osend[d] = whole
            copy = remote(osend.at[d], orecv.at[me], os.at[d], orr.at[d], "fs", seq)
            copy.start()
            returns.append(copy)
        else:
            orecv[me] = whole
    for copy in returns:
        copy.wait_recv()
    for j in range(nfs):
        out_ref[0, :, j * channels : (j + 1) * channels] = orecv[j]
    for copy in shares + swaps + returns:
        copy.wait_send()
    for d in range(2):

        @pl.when(sends[d])
        def _():
            state_copies[d].wait_send()
            halo_copies[d].wait_send()


def shards(
    inputs,
    input_norm_gain,
    receptance_matrix,
    key_matrix,
    value_matrix,
    pooling_input_weight,
    decay_lower_matrix,
    decay_raise_matrix,
    decay_offset_bias,
    removal_lower_matrix,
    removal_raise_matrix,
    removal_rate_bias,
    tempo_scale,
    sudden_decay_extra,
    head_norm_gain,
    group_mixing_weight,
    attention_output_matrix,
    pooling_output_matrix,
):
    nsp, nfs, ntp = lax.axis_size("sp"), lax.axis_size("fs"), lax.axis_size("tp")
    _, tokens, features = inputs.shape
    depth, channels = key_matrix.shape
    pairs = channels // LANES
    heads = channels // HEAD
    dma = pltpu.SemaphoreType.DMA
    limit = 60 * 1024 * 1024
    p4, lat = pl.pallas_call(
        functools.partial(front_kernel, nfs),
        out_shape=(
            jax.ShapeDtypeStruct((4, tokens, channels), bf16),
            jax.ShapeDtypeStruct((2, tokens, decay_lower_matrix.shape[1]), bf16),
        ),
        in_specs=[VMEM] * 8,
        out_specs=(VMEM, VMEM),
        scratch_shapes=[
            pltpu.VMEM((nfs, tokens, depth), bf16),
            pltpu.VMEM((nfs, tokens, depth), bf16),
            pltpu.VMEM((nfs, 4, tokens, channels), bf16),
            pltpu.VMEM((nfs, 4, tokens, channels), bf16),
            dma((nfs,)),
            dma((nfs,)),
            dma((nfs, 4)),
            dma((nfs, 4)),
        ],
        compiler_params=pltpu.CompilerParams(
            collective_id=0, has_side_effects=True, vmem_limit_bytes=limit
        ),
        name="front",
    )(
        inputs,
        input_norm_gain[None],
        receptance_matrix,
        key_matrix,
        value_matrix,
        pooling_input_weight,
        decay_lower_matrix,
        removal_lower_matrix,
    )

    def whole(*shape):
        return pl.BlockSpec(shape, lambda p: (0,) * len(shape))

    rank2 = decay_raise_matrix.shape[0] * decay_raise_matrix.shape[1]
    query, local, transfer, carried = pl.pallas_call(
        mixer_kernel,
        grid=(pairs,),
        out_shape=(
            jax.ShapeDtypeStruct((2, tokens, channels), bf16),
            jax.ShapeDtypeStruct((tokens, channels), f32),
            jax.ShapeDtypeStruct((2, pairs, LANES, LANES), f32),
            jax.ShapeDtypeStruct((2, pairs, HEAD, LANES), f32),
        ),
        in_specs=[
            pl.BlockSpec((4, tokens, LANES), lambda p: (0, 0, p)),
            whole(2, tokens, decay_lower_matrix.shape[1]),
            pl.BlockSpec((rank2, LANES), lambda p: (0, p)),
            pl.BlockSpec((2, LANES), lambda p: (0, p)),
            pl.BlockSpec((rank2, LANES), lambda p: (0, p)),
            pl.BlockSpec((2, LANES), lambda p: (0, p)),
            whole(2, heads, tokens),
            whole(2, heads, tokens),
        ],
        out_specs=(
            pl.BlockSpec((2, tokens, LANES), lambda p: (0, 0, p)),
            pl.BlockSpec((tokens, LANES), lambda p: (0, p)),
            pl.BlockSpec((2, 1, LANES, LANES), lambda p: (0, p, 0, 0)),
            pl.BlockSpec((2, 1, HEAD, LANES), lambda p: (0, p, 0, 0)),
        ),
        compiler_params=pltpu.CompilerParams(
            vmem_limit_bytes=limit, dimension_semantics=("arbitrary",)
        ),
        name="mixer",
    )(
        p4,
        lat,
        decay_raise_matrix.reshape(rank2, channels),
        decay_offset_bias,
        removal_raise_matrix.reshape(rank2, channels),
        removal_rate_bias,
        tempo_scale[0],
        sudden_decay_extra[0],
    )
    return pl.pallas_call(
        functools.partial(tail_kernel, nsp, nfs, ntp),
        out_shape=jax.ShapeDtypeStruct((1, tokens // ntp, features), bf16),
        in_specs=[VMEM] * 9,
        out_specs=VMEM,
        scratch_shapes=[
            pltpu.VMEM((2, HALO, channels), bf16),
            pltpu.VMEM((2, HALO, channels), bf16),
            pltpu.VMEM((2, pairs * HEAD, LANES), bf16),
            pltpu.VMEM((2, pairs * HEAD, LANES), bf16),
            pltpu.VMEM((nfs, 2, tokens, channels), bf16),
            pltpu.VMEM((nfs, tokens // ntp, depth), bf16),
            pltpu.VMEM((nfs, tokens // ntp, depth), bf16),
            pltpu.VMEM((nfs, tokens // ntp, depth), bf16),
            pltpu.VMEM((nfs, tokens // ntp, depth), bf16),
            dma((2,)),
            dma((2,)),
            dma((2,)),
            dma((2,)),
            dma((nfs, 2)),
            dma((nfs, 2)),
            dma((nfs,)),
            dma((nfs,)),
            dma((nfs,)),
            dma((nfs,)),
        ],
        compiler_params=pltpu.CompilerParams(
            collective_id=1, has_side_effects=True, vmem_limit_bytes=limit
        ),
        name="tail",
    )(
        query,
        local,
        transfer,
        carried,
        p4,
        group_mixing_weight,
        head_norm_gain[None],
        attention_output_matrix,
        pooling_output_matrix,
    )


def solution(mesh):
    in_specs = (
        P("fs", "sp", None),
        P(),
        P("fs", "tp"),
        P("fs", "tp"),
        P("fs", "tp"),
        P("fs", "tp"),
        P(),
        P(None, None, "tp"),
        P(None, "tp"),
        P(),
        P(None, None, "tp"),
        P(None, "tp"),
        P("fs", None, "tp", "sp"),
        P("fs", None, "tp", "sp"),
        P("tp"),
        P("tp", None, None),
        P("fs", "tp"),
        P("fs", "tp"),
    )
    out_specs = P("fs", ("sp", "tp"), None)
    return jax.shard_map(shards, mesh=mesh, in_specs=in_specs, out_specs=out_specs, check_vma=False)
```

```python
import functools

import jax
import jax.numpy as jnp
from jax import lax
from jax.experimental import pallas as pl
from jax.experimental.pallas import tpu as pltpu
from jax.sharding import PartitionSpec as P

HEAD = 64
GROUP_WIDTH = 256
LANES = 128
BLOCK = 16
HALO = 16

norm_eps = 1e-06
head_eps = 0.00064
unit_eps = 1e-06
f32 = jnp.float32
bf16 = jnp.bfloat16
VMEM = pl.BlockSpec(memory_space=pltpu.VMEM)


def dot(left, right):
    return jnp.dot(left.astype(bf16), right.astype(bf16), preferred_element_type=f32)


def dot_general(left, right, dims):
    return lax.dot_general(
        left.astype(bf16), right.astype(bf16), (dims, ((), ())), preferred_element_type=f32
    )


def dot_rows(left, right):
    return dot_general(left, right, ((1,), (1,)))


def dot_cols(left, right):
    return dot_general(left, right, ((0,), (0,)))


def exact_dot(left, right, dims):
    return lax.dot_general(
        left, right, (dims, ((), ())), preferred_element_type=f32, precision=lax.Precision.HIGHEST
    )


def remote(src, dst, send, recv, axis, peer):
    return pltpu.make_async_remote_copy(
        src_ref=src,
        dst_ref=dst,
        send_sem=send,
        recv_sem=recv,
        device_id={axis: peer},
        device_id_type=pl.DeviceIdType.MESH,
    )


def greet(barrier, axis, peer):
    pl.semaphore_signal(
        barrier, inc=1, device_id={axis: peer}, device_id_type=pl.DeviceIdType.MESH
    )


def front_part(
    n,
    x_ref,
    gain_ref,
    weights,
    lowers,
    loads,
    pool_ref,
    lat_ref,
    mine,
    cells,
    part,
    pool_part,
    landed,
    pool_landed,
    xs,
    xr,
    ps,
    pr,
    count,
    mix_pair,
):
    me = lax.axis_index("fs")
    width = x_ref.shape[2] // n
    pairs = part.shape[1]
    x = x_ref[0].astype(f32)
    normed = (
        x
        * lax.rsqrt(jnp.mean(x * x, axis=-1, keepdims=True) + norm_eps)
        * gain_ref[...].astype(f32)
    ).astype(bf16)
    for j in range(n):
        mine[j] = normed[:, j * width : (j + 1) * width]
    pl.semaphore_wait(pltpu.get_barrier_semaphore(), count)
    order = [n // 2] + [d for d in range(1, n) if d != n // 2]
    moves = []
    for d in order:
        peer = lax.rem(me + d, n)
        copy = remote(mine.at[peer], cells.at[me], xs.at[d], xr.at[d], "fs", peer)
        copy.start()
        moves.append(copy)
    for load in loads:
        load.wait()
    dl_ref, rl_ref = lowers
    decay = jnp.zeros((x.shape[0], dl_ref.shape[1]), f32)
    rate = jnp.zeros((x.shape[0], rl_ref.shape[1]), f32)
    for j in range(n):
        block = mine[j]
        decay = decay + dot(block, dl_ref[j * width : (j + 1) * width])
        rate = rate + dot(block, rl_ref[j * width : (j + 1) * width])
    lat_ref[0] = jnp.tanh(decay.astype(bf16).astype(f32)).astype(bf16)
    lat_ref[1] = rate.astype(bf16)
    for copy in moves:
        copy.wait_recv()

    def pair_copy(d, p):
        peer = lax.rem(me + d, n)
        return remote(
            part.at[peer, p], landed.at[me, p], ps.at[d, p], pr.at[d, p], "fs", peer
        )

    def pool_copy(d):
        peer = lax.rem(me + d, n)
        return remote(
            pool_part.at[peer],
            pool_landed.at[me],
            ps.at[d, pairs],
            pr.at[d, pairs],
            "fs",
            peer,
        )

    for p in range(pairs):
        for d in order:
            peer = lax.rem(me + d, n)
            for m in range(3):
                part[peer, p, m] = dot(
                    cells[peer], weights[m][:, p * LANES : (p + 1) * LANES]
                ).astype(bf16)
            pair_copy(d, p).start()
    for d in order:
        peer = lax.rem(me + d, n)
        pool_part[peer] = dot(cells[peer], weights[3][...]).astype(bf16)
        pool_copy(d).start()

    def pair_step(p, carry):
        lanes = pl.ds(pl.multiple_of(p * LANES, LANES), LANES)
        owned = [dot(mine[me], weights[m][:, lanes]) for m in range(3)]
        for d in range(1, n):
            pair_copy(d, p).wait_recv()
        for d in range(1, n):
            peer = lax.rem(me + d, n)
            owned = [o + landed[peer, p, m].astype(f32) for m, o in enumerate(owned)]
        mix_pair(p, lanes, *[o.astype(bf16) for o in owned])
        return carry

    lax.fori_loop(0, pairs, pair_step, 0)
    total = dot(mine[me], weights[3][...])
    for d in range(1, n):
        pool_copy(d).wait_recv()
    for d in range(1, n):
        total = total + pool_landed[lax.rem(me + d, n)].astype(f32)
    pool_ref[...] = total.astype(bf16)
    for copy in moves:
        copy.wait_send()
    for d in range(1, n):
        for p in range(pairs):
            pair_copy(d, p).wait_send()
        pool_copy(d).wait_send()


def mix_pair(
    pair,
    lanes,
    key,
    receptance,
    value,
    lat_ref,
    draise_ref,
    dbias_ref,
    rraise_ref,
    rbias_ref,
    tempo_ref,
    extra_ref,
    query_ref,
    local_ref,
    transfer_ref,
    carried_ref,
):
    tokens = key.shape[0]
    kf = key.astype(f32)
    rf = receptance.astype(f32)
    lane = lax.broadcasted_iota(jnp.int32, (tokens, LANES), 1)
    row = lax.broadcasted_iota(jnp.int32, (tokens, LANES), 0)
    head0 = lane < HEAD
    k2 = kf * kf
    s0 = jnp.sum(jnp.where(head0, k2, 0.0), axis=-1, keepdims=True)
    s1 = jnp.sum(jnp.where(head0, 0.0, k2), axis=-1, keepdims=True)
    unit = kf * lax.rsqrt(jnp.where(head0, s0, s1) + unit_eps)
    heads = tempo_ref.shape[1]
    spread = (
        lax.broadcasted_iota(jnp.int32, (heads, LANES), 0)
        == 2 * pair + lax.broadcasted_iota(jnp.int32, (heads, LANES), 1) // HEAD
    ).astype(f32)
    blocks = tokens // BLOCK
    zero_row = jnp.zeros((1, LANES), f32)
    eye = (row == lane).astype(f32)
    sizes = []
    size = 1
    while size < tokens:
        sizes.append(size)
        size *= 2

    def level_mask(k):
        return ((row >> (k + 1)) == (lane >> (k + 1))) & ((row >> k) != (lane >> k))

    ways = []
    for d in range(2):
        lat_mask = head0 if d == 0 else ~head0
        lat_d = jnp.where(lat_mask, lat_ref[0].astype(f32), 0.0)
        lat_r = jnp.where(lat_mask, lat_ref[1].astype(f32), 0.0)
        pre = dbias_ref[d : d + 1, lanes] + dot(lat_d, draise_ref[:, lanes])
        velocity = jax.nn.sigmoid(pre) * 0.6065306597126334
        tempo = exact_dot(tempo_ref[d], spread, ((0,), (0,)))
        extra = exact_dot(extra_ref[d], spread, ((0,), (0,)))
        ld = -velocity * tempo + extra
        rate = jax.nn.sigmoid(rbias_ref[d : d + 1, lanes] + dot(lat_r, rraise_ref[:, lanes]))
        removal = unit * rate
        written = kf * rate
        upto = (lane <= row) if d == 0 else (lane >= row)
        inner = exact_dot(upto.astype(f32), ld, ((1,), (0,)))
        excl = inner - ld
        grams = []
        for i in range(blocks):
            lo, hi = i * BLOCK, (i + 1) * BLOCK
            if d == 0:
                base = inner[lo - 1 : lo] if i > 0 else zero_row
            else:
                base = inner[hi : hi + 1] if i < blocks - 1 else zero_row
            ahead = unit[lo:hi] * jnp.exp(excl[lo:hi] - base)
            query = rf[lo:hi] * jnp.exp(inner[lo:hi] - base)
            grow = jnp.exp(jnp.minimum(base - inner, 80.0))
            right = jnp.concatenate([(removal * grow).astype(bf16), (written * grow).astype(bf16)], 0)
            h0 = head0[lo:hi]
            left = jnp.concatenate(
                [
                    jnp.where(h0, ahead, 0.0),
                    jnp.where(h0, 0.0, ahead),
                    jnp.where(h0, query, 0.0),
                    jnp.where(h0, 0.0, query),
                ],
                0,
            )
            grams.append(dot_rows(left, right))
        strict = (lane < row) if d == 0 else (lane > row)

        def gathered(place, at, mask):
            rows = jnp.concatenate(
                [g[place * BLOCK : (place + 1) * BLOCK, at * tokens : (at + 1) * tokens] for g in grams],
                0,
            )
            return jnp.where(mask, rows, 0.0)

        way = dict(inner=inner, excl=excl, removal=removal, written=written)
        way["link"] = [gathered(h, 0, strict) for h in range(2)]
        way["link_write"] = [gathered(h, 1, strict).astype(bf16) for h in range(2)]
        way["read"] = [gathered(2 + h, 0, upto).astype(bf16) for h in range(2)]
        way["read_write"] = [gathered(2 + h, 1, upto).astype(bf16) for h in range(2)]
        ways.append(way)

    links = [way["link"][h] for way in ways for h in range(2)]
    inverses = [eye - jnp.where(level_mask(0), a, 0.0) for a in links]
    for k in range(1, len(sizes)):
        mask = level_mask(k)
        firsts = [dot(t, jnp.where(mask, a, 0.0)) for t, a in zip(inverses, links)]
        inverses = [t - dot(u, t) for t, u in zip(inverses, firsts)]

    block_diag = (row < HEAD) == head0
    local = jnp.zeros((tokens, LANES), f32)
    for d, way in enumerate(ways):
        inner, excl = way["inner"], way["excl"]
        last = inner[tokens - 1 : tokens] if d == 0 else inner[0:1]
        ahead = unit * jnp.exp(excl)
        query = rf * jnp.exp(inner)
        tail = jnp.exp(last - inner)

        def chosen(pieces):
            return jnp.where(head0, pieces[0], pieces[1])

        base = chosen([dot(way["link_write"][h], value) for h in range(2)])
        rhs = jnp.concatenate([ahead.astype(bf16), base.astype(bf16)], 1)
        solved = [dot(inverses[2 * d + h], rhs) for h in range(2)]
        pull_map = -chosen([s[:, :LANES] for s in solved])
        pull_base = -chosen([s[:, LANES:] for s in solved])
        remove_tail = (way["removal"] * tail).astype(bf16)
        write_tail = (way["written"] * tail).astype(bf16)
        both = jnp.concatenate([pull_map.astype(bf16), pull_base.astype(bf16)], 1)
        seen = [dot(way["read"][h], both) for h in range(2)]
        query_ref[d, :, lanes] = (query + chosen([s[:, :LANES] for s in seen])).astype(bf16)
        local = (
            local
            + chosen([s[:, LANES:] for s in seen])
            + chosen([dot(way["read_write"][h], value) for h in range(2)])
        )
        transfer = jnp.where(block_diag, dot_cols(pull_map, remove_tail), 0.0) + eye * jnp.exp(last)
        transfer_ref[d, pair] = transfer
        carried = dot_cols(
            jnp.concatenate([pull_base.astype(bf16), value], 0),
            jnp.concatenate([remove_tail, write_tail], 0),
        )
        carried = jnp.where(block_diag, carried, 0.0)
        carried_ref[d, pair] = carried[:HEAD] + carried[HEAD:]
    local_ref[:, lanes] = local


def layer_kernel(
    nsp,
    nfs,
    ntp,
    x_ref,
    in_gain_ref,
    wk_hbm,
    wr_hbm,
    wv_hbm,
    wi_hbm,
    dl_hbm,
    rl_hbm,
    draise_ref,
    dbias_ref,
    rraise_ref,
    rbias_ref,
    tempo_ref,
    extra_ref,
    mix_hbm,
    gain_ref,
    wa_hbm,
    wp_hbm,
    out_ref,
    wk_ref,
    wr_ref,
    wv_ref,
    wi_ref,
    dl_ref,
    rl_ref,
    mix_ref,
    wa_ref,
    wp_ref,
    loaded,
    mine,
    cells,
    part,
    pool_part,
    landed,
    pool_landed,
    xs,
    xr,
    ps,
    pr,
    lat_ref,
    pool_ref,
    query_ref,
    local_ref,
    transfer_ref,
    carried_ref,
    edge,
    halo,
    incoming,
    leaving,
    act,
    tsend,
    trecv,
    osend,
    orecv,
    hs,
    hr,
    ss,
    sr,
    gs,
    gr,
    ts,
    tr,
    os,
    orr,
):
    z = lax.axis_index("sp")
    me = lax.axis_index("fs")
    core = lax.axis_index("tp")
    tokens, channels = local_ref.shape
    pairs = transfer_ref.shape[1]
    half_rows = tokens // ntp
    has_prev = z > 0
    has_next = z < nsp - 1
    prev = jnp.maximum(z - 1, 0)
    after = jnp.minimum(z + 1, nsp - 1)

    barrier = pltpu.get_barrier_semaphore()
    for d in range(1, nfs):
        greet(barrier, "fs", lax.rem(me + d, nfs))
    for d in range(1, ntp):
        greet(barrier, "tp", lax.rem(core + d, ntp))
    pl.when(has_prev)(lambda: greet(barrier, "sp", prev))
    pl.when(has_next)(lambda: greet(barrier, "sp", after))
    count = nfs + ntp - 2 + jnp.where(has_prev, 1, 0) + jnp.where(has_next, 1, 0)
    sources = (dl_hbm, rl_hbm, wk_hbm, wr_hbm, wv_hbm, wi_hbm, mix_hbm, wa_hbm, wp_hbm)
    targets = (dl_ref, rl_ref, wk_ref, wr_ref, wv_ref, wi_ref, mix_ref, wa_ref, wp_ref)
    loads = [
        pltpu.make_async_copy(source, target, loaded.at[i])
        for i, (source, target) in enumerate(zip(sources, targets))
    ]
    for load in loads:
        load.start()
    front_part(
        nfs,
        x_ref,
        in_gain_ref,
        (wk_ref, wr_ref, wv_ref, wi_ref),
        (dl_ref, rl_ref),
        loads[:6],
        pool_ref,
        lat_ref,
        mine,
        cells,
        part,
        pool_part,
        landed,
        pool_landed,
        xs,
        xr,
        ps,
        pr,
        count,
        lambda pair, lanes, key, receptance, value: mix_pair(
            pair,
            lanes,
            key,
            receptance,
            value,
            lat_ref,
            draise_ref,
            dbias_ref,
            rraise_ref,
            rbias_ref,
            tempo_ref,
            extra_ref,
            query_ref,
            local_ref,
            transfer_ref,
            carried_ref,
        ),
    )
    for load in loads[6:]:
        load.wait()
    edge[0] = pool_ref[:HALO]
    edge[1] = pool_ref[tokens - HALO :]

    sides = [(has_prev, prev, has_next), (has_next, after, has_prev)]
    def state_copy(d, p):
        return remote(
            leaving.at[d, p],
            incoming.at[d, p],
            ss.at[d, p],
            sr.at[d, p],
            "sp",
            after if d == 0 else prev,
        )

    halo_copies = [
        remote(edge.at[1], halo.at[0], hs.at[0], hr.at[0], "sp", after),
        remote(edge.at[0], halo.at[1], hs.at[1], hr.at[1], "sp", prev),
    ]
    sends = [has_next, has_prev]
    takes = [has_prev, has_next]

    def relay(d):
        @pl.when(jnp.logical_not(takes[d]))
        def _():
            incoming[d] = jnp.zeros_like(incoming[d])

        for p in range(pairs):

            @pl.when(takes[d])
            def _():
                state_copy(d, p).wait_recv()

            @pl.when(sends[d])
            def _():
                leaving[d, p] = (
                    dot(incoming[d, p], transfer_ref[d, p]) + carried_ref[d, p]
                ).astype(bf16)
                state_copy(d, p).start()

    def start_halo(d):
        pl.when(sends[d])(lambda: halo_copies[d].start())

    early = 2 * z < nsp

    @pl.when(early)
    def _():
        relay(0)

    @pl.when(jnp.logical_not(early))
    def _():
        relay(1)

    for d in range(2):
        start_halo(d)
    for d in range(2):

        @pl.when(takes[d])
        def _():
            halo_copies[d].wait_recv()

        @pl.when(jnp.logical_not(takes[d]))
        def _():
            halo[d] = jnp.zeros_like(halo[d])

    span = tokens + 2 * HALO
    rim = jnp.concatenate([halo[0], pool_ref[...], halo[1]], 0)
    here = lax.broadcasted_iota(jnp.int32, (tokens, span), 0)
    there = lax.broadcasted_iota(jnp.int32, (tokens, span), 1) - HALO
    position = z * tokens + lax.broadcasted_iota(jnp.int32, (tokens, GROUP_WIDTH), 0)
    length = tokens * nsp
    groups_here = channels // GROUP_WIDTH
    for member in range(groups_here):
        cols = slice(member * GROUP_WIDTH, (member + 1) * GROUP_WIDTH)
        reach = jnp.left_shift(1, core * groups_here + member)
        window = jnp.where((there >= here - reach) & (there < here + reach), 1.0, 0.0)
        total = dot(window, rim[:, cols])
        size = (
            jnp.minimum(position + reach, length) - jnp.maximum(position - reach, 0)
        ).astype(f32)
        diff = (total / size - pool_ref[:, cols].astype(f32)).astype(bf16)
        act[me, 0, :, cols] = dot(diff, mix_ref[member]).astype(bf16)
    order = [nfs // 2] + [d for d in range(1, nfs) if d != nfs // 2]
    shares = []
    for d in order:
        peer = lax.rem(me + d, nfs)
        copy = remote(act.at[me, 0], act.at[me, 0], gs.at[d, 0], gr.at[d, 0], "fs", peer)
        copy.start()
        shares.append(copy)

    @pl.when(early)
    def _():
        relay(1)

    @pl.when(jnp.logical_not(early))
    def _():
        relay(0)

    head0 = lax.broadcasted_iota(jnp.int32, (tokens, LANES), 1) < HEAD
    top0 = lax.broadcasted_iota(jnp.int32, (HEAD, LANES), 1) < HEAD
    for p in range(pairs):
        lanes = slice(p * LANES, (p + 1) * LANES)
        readout = local_ref[:, lanes]
        for d in range(2):
            state = incoming[d, p].astype(f32)
            wide = jnp.concatenate(
                [jnp.where(top0, state, 0.0), jnp.where(top0, 0.0, state)], 0
            )
            readout = readout + dot_rows(query_ref[d, :, lanes], wide)

        def head_mean(cells):
            low = jnp.sum(jnp.where(head0, cells, 0.0), axis=-1, keepdims=True)
            high = jnp.sum(jnp.where(head0, 0.0, cells), axis=-1, keepdims=True)
            return jnp.where(head0, low, high) * (1.0 / HEAD)

        centred = readout - head_mean(readout)
        scaled = centred * lax.rsqrt(head_mean(centred * centred) + head_eps)
        act[me, 1, :, lanes] = (scaled * gain_ref[:, lanes].astype(f32)).astype(bf16)
    for d in order:
        peer = lax.rem(me + d, nfs)
        copy = remote(act.at[me, 1], act.at[me, 1], gs.at[d, 1], gr.at[d, 1], "fs", peer)
        copy.start()
        shares.append(copy)

    other = lax.rem(core + 1, ntp)
    mine_at = pl.multiple_of(core * half_rows, half_rows)
    other_at = pl.multiple_of(other * half_rows, half_rows)

    def product(seq, rows):
        return dot_rows(act[seq, 1, rows], wa_ref[...]) + dot_rows(act[seq, 0, rows], wp_ref[...])

    returns = []
    swaps = []
    turns = [0] + [d for d in range(1, nfs) if d != nfs // 2] + [nfs // 2]
    for d in turns:
        seq = lax.rem(me + nfs - d, nfs)
        if d:
            for copy, at in zip(shares, order + order):
                if at == d:
                    copy.wait_recv()
        tsend[d] = product(seq, pl.ds(other_at, half_rows)).astype(bf16)
        swap = remote(tsend.at[d], trecv.at[d], ts.at[d], tr.at[d], "tp", other)
        swap.start()
        swaps.append(swap)
        kept = product(seq, pl.ds(mine_at, half_rows))
        swap.wait_recv()
        whole = (kept + trecv[d].astype(f32)).astype(bf16)
        if d:
            osend[d] = whole
            copy = remote(osend.at[d], orecv.at[me], os.at[d], orr.at[d], "fs", seq)
            copy.start()
            returns.append(copy)
        else:
            orecv[me] = whole
    for copy in returns:
        copy.wait_recv()
    for j in range(nfs):
        out_ref[0, :, j * channels : (j + 1) * channels] = orecv[j]
    for copy in shares + swaps + returns:
        copy.wait_send()
    for d in range(2):

        @pl.when(sends[d])
        def _():
            for p in range(pairs):
                state_copy(d, p).wait_send()
            halo_copies[d].wait_send()


def shards(
    inputs,
    input_norm_gain,
    receptance_matrix,
    key_matrix,
    value_matrix,
    pooling_input_weight,
    decay_lower_matrix,
    decay_raise_matrix,
    decay_offset_bias,
    removal_lower_matrix,
    removal_raise_matrix,
    removal_rate_bias,
    tempo_scale,
    sudden_decay_extra,
    head_norm_gain,
    group_mixing_weight,
    attention_output_matrix,
    pooling_output_matrix,
):
    nsp, nfs, ntp = lax.axis_size("sp"), lax.axis_size("fs"), lax.axis_size("tp")
    _, tokens, features = inputs.shape
    depth, channels = key_matrix.shape
    pairs = channels // LANES
    dma = pltpu.SemaphoreType.DMA
    rank = decay_lower_matrix.shape[1]
    rank2 = decay_raise_matrix.shape[0] * decay_raise_matrix.shape[1]
    anywhere = pl.BlockSpec(memory_space=pl.ANY)
    half = (nfs, tokens // ntp, depth)
    return pl.pallas_call(
        functools.partial(layer_kernel, nsp, nfs, ntp),
        out_shape=jax.ShapeDtypeStruct((1, tokens // ntp, features), bf16),
        in_specs=[VMEM] * 2
        + [anywhere] * 6
        + [VMEM] * 6
        + [anywhere, VMEM, anywhere, anywhere],
        out_specs=VMEM,
        scratch_shapes=[pltpu.VMEM((depth, channels), bf16)] * 4
        + [
            pltpu.VMEM((features, rank), bf16),
            pltpu.VMEM((features, rank), bf16),
            pltpu.VMEM(group_mixing_weight.shape, bf16),
            pltpu.VMEM(attention_output_matrix.shape, bf16),
            pltpu.VMEM(pooling_output_matrix.shape, bf16),
            dma((9,)),
            pltpu.VMEM((nfs, tokens, depth), bf16),
            pltpu.VMEM((nfs, tokens, depth), bf16),
            pltpu.VMEM((nfs, pairs, 3, tokens, LANES), bf16),
            pltpu.VMEM((nfs, tokens, channels), bf16),
            pltpu.VMEM((nfs, pairs, 3, tokens, LANES), bf16),
            pltpu.VMEM((nfs, tokens, channels), bf16),
            dma((nfs,)),
            dma((nfs,)),
            dma((nfs, pairs + 1)),
            dma((nfs, pairs + 1)),
            pltpu.VMEM((2, tokens, rank), bf16),
            pltpu.VMEM((tokens, channels), bf16),
            pltpu.VMEM((2, tokens, channels), bf16),
            pltpu.VMEM((tokens, channels), f32),
            pltpu.VMEM((2, pairs, LANES, LANES), f32),
            pltpu.VMEM((2, pairs, HEAD, LANES), f32),
            pltpu.VMEM((2, HALO, channels), bf16),
            pltpu.VMEM((2, HALO, channels), bf16),
            pltpu.VMEM((2, pairs, HEAD, LANES), bf16),
            pltpu.VMEM((2, pairs, HEAD, LANES), bf16),
            pltpu.VMEM((nfs, 2, tokens, channels), bf16),
            pltpu.VMEM(half, bf16),
            pltpu.VMEM(half, bf16),
            pltpu.VMEM(half, bf16),
            pltpu.VMEM(half, bf16),
            dma((2,)),
            dma((2,)),
            dma((2, pairs)),
            dma((2, pairs)),
            dma((nfs, 2)),
            dma((nfs, 2)),
            dma((nfs,)),
            dma((nfs,)),
            dma((nfs,)),
            dma((nfs,)),
        ],
        compiler_params=pltpu.CompilerParams(
            collective_id=0, has_side_effects=True, vmem_limit_bytes=60 * 1024 * 1024
        ),
        name="layer",
    )(
        inputs,
        input_norm_gain[None],
        key_matrix,
        receptance_matrix,
        value_matrix,
        pooling_input_weight,
        decay_lower_matrix,
        removal_lower_matrix,
        decay_raise_matrix.reshape(rank2, channels),
        decay_offset_bias,
        removal_raise_matrix.reshape(rank2, channels),
        removal_rate_bias,
        tempo_scale[0],
        sudden_decay_extra[0],
        group_mixing_weight,
        head_norm_gain[None],
        attention_output_matrix,
        pooling_output_matrix,
    )


def solution(mesh):
    in_specs = (
        P("fs", "sp", None),
        P(),
        P("fs", "tp"),
        P("fs", "tp"),
        P("fs", "tp"),
        P("fs", "tp"),
        P(),
        P(None, None, "tp"),
        P(None, "tp"),
        P(),
        P(None, None, "tp"),
        P(None, "tp"),
        P("fs", None, "tp", "sp"),
        P("fs", None, "tp", "sp"),
        P("tp"),
        P("tp", None, None),
        P("fs", "tp"),
        P("fs", "tp"),
    )
    out_specs = P("fs", ("sp", "tp"), None)
    return jax.shard_map(shards, mesh=mesh, in_specs=in_specs, out_specs=out_specs, check_vma=False)
```

```python
import functools

import jax
import jax.numpy as jnp
from jax import lax
from jax.experimental import pallas as pl
from jax.experimental.pallas import tpu as pltpu
from jax.sharding import PartitionSpec as P

HEAD = 64
GROUP_WIDTH = 256
LANES = 128
BLOCK = 16
HALO = 16

norm_eps = 1e-06
head_eps = 0.00064
unit_eps = 1e-06
f32 = jnp.float32
bf16 = jnp.bfloat16
VMEM = pl.BlockSpec(memory_space=pltpu.VMEM)


def dot(left, right):
    return jnp.dot(left.astype(bf16), right.astype(bf16), preferred_element_type=f32)


def dot_general(left, right, dims):
    return lax.dot_general(
        left.astype(bf16), right.astype(bf16), (dims, ((), ())), preferred_element_type=f32
    )


def dot_rows(left, right):
    return dot_general(left, right, ((1,), (1,)))


def dot_cols(left, right):
    return dot_general(left, right, ((0,), (0,)))


def exact_dot(left, right, dims):
    return lax.dot_general(
        left, right, (dims, ((), ())), preferred_element_type=f32, precision=lax.Precision.HIGHEST
    )


def remote(src, dst, send, recv, axis, peer):
    return pltpu.make_async_remote_copy(
        src_ref=src,
        dst_ref=dst,
        send_sem=send,
        recv_sem=recv,
        device_id={axis: peer},
        device_id_type=pl.DeviceIdType.MESH,
    )


def greet(barrier, axis, peer):
    pl.semaphore_signal(
        barrier, inc=1, device_id={axis: peer}, device_id_type=pl.DeviceIdType.MESH
    )


def flipped(at, bits):
    moved = at
    bit = 1
    while bit <= bits:
        if bits & bit:
            moved = moved + bit - 2 * bit * lax.rem(at // bit, 2)
        bit *= 2
    return moved


def front_part(
    n,
    x_ref,
    gain_ref,
    weights,
    lowers,
    loads,
    pool_ref,
    lat_ref,
    mine,
    cells,
    part,
    pool_part,
    landed,
    pool_landed,
    xs,
    xr,
    ps,
    pr,
    count,
    mix_pair,
):
    me = lax.axis_index("fs")
    core, ntp = lax.axis_index("tp"), lax.axis_size("tp")
    width = x_ref.shape[2] // n
    share = x_ref.shape[1] // ntp
    rows = pl.ds(pl.multiple_of(core * share, share), share)
    pairs = part.shape[1]
    x = x_ref[0].astype(f32)
    normed = (
        x
        * lax.rsqrt(jnp.mean(x * x, axis=-1, keepdims=True) + norm_eps)
        * gain_ref[...].astype(f32).reshape(1, -1)
    ).astype(bf16)
    for j in range(n):
        mine[j] = normed[:, j * width : (j + 1) * width]
    pl.semaphore_wait(pltpu.get_barrier_semaphore(), count)
    order = list(range(n - 1, 0, -1))
    moves = []
    for d in order:
        peer = flipped(me, d)
        copy = remote(
            mine.at[peer, rows], cells.at[me, rows], xs.at[d, 0], xr.at[d, 0], "fs", peer
        )
        copy.start()
        moves.append(copy)
    for load in loads[:2]:
        load.wait()
    dl_ref, rl_ref = lowers
    decay = jnp.zeros((x.shape[0], dl_ref.shape[1]), f32)
    rate = jnp.zeros((x.shape[0], rl_ref.shape[1]), f32)
    for j in range(n):
        block = mine[j]
        decay = decay + dot(block, dl_ref[j * width : (j + 1) * width])
        rate = rate + dot(block, rl_ref[j * width : (j + 1) * width])
    lat_ref[0] = jnp.tanh(decay.astype(bf16).astype(f32)).astype(bf16)
    lat_ref[1] = rate.astype(bf16)
    for load in loads[2:]:
        load.wait()
    for d, copy in zip(order, list(moves)):
        peer = flipped(me, d)
        copy.wait_recv()
        for e in range(1, ntp):
            passed = remote(
                cells.at[peer, rows],
                cells.at[peer, rows],
                xs.at[d, e],
                xr.at[d, e],
                "tp",
                lax.rem(core + e, ntp),
            )
            passed.start()
            moves.append(passed)
    for copy in moves[len(order) :]:
        copy.wait_recv()

    def pair_copy(d, p):
        peer = flipped(me, d)
        return remote(
            part.at[peer, p], landed.at[me, p], ps.at[d, p], pr.at[d, p], "fs", peer
        )

    def pool_copy(d):
        peer = flipped(me, d)
        return remote(
            pool_part.at[peer],
            pool_landed.at[me],
            ps.at[d, pairs],
            pr.at[d, pairs],
            "fs",
            peer,
        )

    for p in range(pairs):
        for d in order:
            peer = flipped(me, d)
            for m in range(3):
                part[peer, p, m] = dot(
                    cells[peer], weights[m][:, p * LANES : (p + 1) * LANES]
                ).astype(bf16)
            pair_copy(d, p).start()
    for d in order:
        peer = flipped(me, d)
        pool_part[peer] = dot(cells[peer], weights[3][...]).astype(bf16)
        pool_copy(d).start()

    def pair_step(p, carry):
        lanes = pl.ds(pl.multiple_of(p * LANES, LANES), LANES)
        owned = [dot(mine[me], weights[m][:, lanes]) for m in range(3)]
        for d in range(1, n):
            pair_copy(d, p).wait_recv()
        for d in range(1, n):
            peer = flipped(me, d)
            owned = [o + landed[peer, p, m].astype(f32) for m, o in enumerate(owned)]
        mix_pair(p, lanes, *[o.astype(bf16) for o in owned])
        return carry

    lax.fori_loop(0, pairs, pair_step, 0)
    total = dot(mine[me], weights[3][...])
    for d in range(1, n):
        pool_copy(d).wait_recv()
    for d in range(1, n):
        total = total + pool_landed[flipped(me, d)].astype(f32)
    pool_ref[...] = total.astype(bf16)
    for copy in moves:
        copy.wait_send()
    for d in range(1, n):
        for p in range(pairs):
            pair_copy(d, p).wait_send()
        pool_copy(d).wait_send()


def mix_pair(
    pair,
    lanes,
    key,
    receptance,
    value,
    lat_ref,
    draise_ref,
    dbias_ref,
    rraise_ref,
    rbias_ref,
    tempo_ref,
    extra_ref,
    query_ref,
    local_ref,
    transfer_ref,
    carried_ref,
):
    tokens = key.shape[0]
    kf = key.astype(f32)
    rf = receptance.astype(f32)
    lane = lax.broadcasted_iota(jnp.int32, (tokens, LANES), 1)
    row = lax.broadcasted_iota(jnp.int32, (tokens, LANES), 0)
    head0 = lane < HEAD
    k2 = kf * kf
    s0 = jnp.sum(jnp.where(head0, k2, 0.0), axis=-1, keepdims=True)
    s1 = jnp.sum(jnp.where(head0, 0.0, k2), axis=-1, keepdims=True)
    unit = kf * lax.rsqrt(jnp.where(head0, s0, s1) + unit_eps)
    heads = tempo_ref.shape[1]
    spread = (
        lax.broadcasted_iota(jnp.int32, (heads, LANES), 0)
        == 2 * pair + lax.broadcasted_iota(jnp.int32, (heads, LANES), 1) // HEAD
    ).astype(f32)
    blocks = tokens // BLOCK
    zero_row = jnp.zeros((1, LANES), f32)
    eye = (row == lane).astype(f32)
    sizes = []
    size = 1
    while size < tokens:
        sizes.append(size)
        size *= 2

    def level_mask(k):
        return ((row >> (k + 1)) == (lane >> (k + 1))) & ((row >> k) != (lane >> k))

    ways = []
    for d in range(2):
        lat_mask = head0 if d == 0 else ~head0
        lat_d = jnp.where(lat_mask, lat_ref[0].astype(f32), 0.0)
        lat_r = jnp.where(lat_mask, lat_ref[1].astype(f32), 0.0)
        pre = dbias_ref[d : d + 1, lanes] + dot(lat_d, draise_ref[:, lanes])
        velocity = jax.nn.sigmoid(pre) * 0.6065306597126334
        tempo = exact_dot(tempo_ref[d], spread, ((0,), (0,)))
        extra = exact_dot(extra_ref[d], spread, ((0,), (0,)))
        ld = -velocity * tempo + extra
        rate = jax.nn.sigmoid(rbias_ref[d : d + 1, lanes] + dot(lat_r, rraise_ref[:, lanes]))
        removal = unit * rate
        written = kf * rate
        upto = (lane <= row) if d == 0 else (lane >= row)
        inner = exact_dot(upto.astype(f32), ld, ((1,), (0,)))
        excl = inner - ld
        grams = []
        for i in range(blocks):
            lo, hi = i * BLOCK, (i + 1) * BLOCK
            if d == 0:
                base = inner[lo - 1 : lo] if i > 0 else zero_row
            else:
                base = inner[hi : hi + 1] if i < blocks - 1 else zero_row
            ahead = unit[lo:hi] * jnp.exp(excl[lo:hi] - base)
            query = rf[lo:hi] * jnp.exp(inner[lo:hi] - base)
            grow = jnp.exp(jnp.minimum(base - inner, 80.0))
            right = jnp.concatenate([(removal * grow).astype(bf16), (written * grow).astype(bf16)], 0)
            h0 = head0[lo:hi]
            left = jnp.concatenate(
                [
                    jnp.where(h0, ahead, 0.0),
                    jnp.where(h0, 0.0, ahead),
                    jnp.where(h0, query, 0.0),
                    jnp.where(h0, 0.0, query),
                ],
                0,
            )
            grams.append(dot_rows(left, right))
        strict = (lane < row) if d == 0 else (lane > row)

        def gathered(place, at, mask):
            rows = jnp.concatenate(
                [g[place * BLOCK : (place + 1) * BLOCK, at * tokens : (at + 1) * tokens] for g in grams],
                0,
            )
            return jnp.where(mask, rows, 0.0)

        way = dict(inner=inner, excl=excl, removal=removal, written=written)
        way["link"] = [gathered(h, 0, strict) for h in range(2)]
        way["link_write"] = [gathered(h, 1, strict).astype(bf16) for h in range(2)]
        way["read"] = [gathered(2 + h, 0, upto).astype(bf16) for h in range(2)]
        way["read_write"] = [gathered(2 + h, 1, upto).astype(bf16) for h in range(2)]
        ways.append(way)

    links = [way["link"][h] for way in ways for h in range(2)]
    inverses = [eye - jnp.where(level_mask(0), a, 0.0) for a in links]
    for k in range(1, len(sizes)):
        mask = level_mask(k)
        firsts = [dot(t, jnp.where(mask, a, 0.0)) for t, a in zip(inverses, links)]
        inverses = [t - dot(u, t) for t, u in zip(inverses, firsts)]

    block_diag = (row < HEAD) == head0
    local = jnp.zeros((tokens, LANES), f32)
    for d, way in enumerate(ways):
        inner, excl = way["inner"], way["excl"]
        last = inner[tokens - 1 : tokens] if d == 0 else inner[0:1]
        ahead = unit * jnp.exp(excl)
        query = rf * jnp.exp(inner)
        tail = jnp.exp(last - inner)

        def chosen(pieces):
            return jnp.where(head0, pieces[0], pieces[1])

        base = chosen([dot(way["link_write"][h], value) for h in range(2)])
        rhs = jnp.concatenate([ahead.astype(bf16), base.astype(bf16)], 1)
        solved = [dot(inverses[2 * d + h], rhs) for h in range(2)]
        pull_map = -chosen([s[:, :LANES] for s in solved])
        pull_base = -chosen([s[:, LANES:] for s in solved])
        remove_tail = (way["removal"] * tail).astype(bf16)
        write_tail = (way["written"] * tail).astype(bf16)
        both = jnp.concatenate([pull_map.astype(bf16), pull_base.astype(bf16)], 1)
        seen = [dot(way["read"][h], both) for h in range(2)]
        query_ref[d, :, lanes] = (query + chosen([s[:, :LANES] for s in seen])).astype(bf16)
        local = (
            local
            + chosen([s[:, LANES:] for s in seen])
            + chosen([dot(way["read_write"][h], value) for h in range(2)])
        )
        transfer = jnp.where(block_diag, dot_cols(pull_map, remove_tail), 0.0) + eye * jnp.exp(last)
        transfer_ref[d, pair] = transfer
        carried = dot_cols(
            jnp.concatenate([pull_base.astype(bf16), value], 0),
            jnp.concatenate([remove_tail, write_tail], 0),
        )
        carried = jnp.where(block_diag, carried, 0.0)
        carried_ref[d, pair] = carried[:HEAD] + carried[HEAD:]
    local_ref[:, lanes] = local


def layer_kernel(
    nsp,
    nfs,
    ntp,
    x_ref,
    in_gain_ref,
    wk_hbm,
    wr_hbm,
    wv_hbm,
    wi_hbm,
    dl_hbm,
    rl_hbm,
    draise_ref,
    dbias_ref,
    rraise_ref,
    rbias_ref,
    tempo_ref,
    extra_ref,
    mix_hbm,
    gain_ref,
    wa_hbm,
    wp_hbm,
    out_ref,
    wk_ref,
    wr_ref,
    wv_ref,
    wi_ref,
    dl_ref,
    rl_ref,
    mix_ref,
    wa_ref,
    wp_ref,
    loaded,
    mine,
    cells,
    part,
    pool_part,
    landed,
    pool_landed,
    xs,
    xr,
    ps,
    pr,
    lat_ref,
    pool_ref,
    query_ref,
    local_ref,
    transfer_ref,
    carried_ref,
    edge,
    halo,
    incoming,
    leaving,
    act,
    tsend,
    trecv,
    osend,
    orecv,
    hs,
    hr,
    ss,
    sr,
    gs,
    gr,
    ts,
    tr,
    os,
    orr,
):
    z = lax.axis_index("sp")
    me = lax.axis_index("fs")
    core = lax.axis_index("tp")
    tokens, channels = local_ref.shape
    pairs = transfer_ref.shape[1]
    half_rows = tokens // ntp
    has_prev = z > 0
    has_next = z < nsp - 1
    prev = jnp.maximum(z - 1, 0)
    after = jnp.minimum(z + 1, nsp - 1)

    barrier = pltpu.get_barrier_semaphore()
    for d in range(1, nfs):
        greet(barrier, "fs", flipped(me, d))
    for d in range(1, ntp):
        greet(barrier, "tp", lax.rem(core + d, ntp))
    pl.when(has_prev)(lambda: greet(barrier, "sp", prev))
    pl.when(has_next)(lambda: greet(barrier, "sp", after))
    count = nfs + ntp - 2 + jnp.where(has_prev, 1, 0) + jnp.where(has_next, 1, 0)
    sources = (dl_hbm, rl_hbm, wk_hbm, wr_hbm, wv_hbm, wi_hbm, mix_hbm, wa_hbm, wp_hbm)
    targets = (dl_ref, rl_ref, wk_ref, wr_ref, wv_ref, wi_ref, mix_ref, wa_ref, wp_ref)
    loads = [
        pltpu.make_async_copy(source, target, loaded.at[i])
        for i, (source, target) in enumerate(zip(sources, targets))
    ]
    for load in loads:
        load.start()
    front_part(
        nfs,
        x_ref,
        in_gain_ref,
        (wk_ref, wr_ref, wv_ref, wi_ref),
        (dl_ref, rl_ref),
        loads[:6],
        pool_ref,
        lat_ref,
        mine,
        cells,
        part,
        pool_part,
        landed,
        pool_landed,
        xs,
        xr,
        ps,
        pr,
        count,
        lambda pair, lanes, key, receptance, value: mix_pair(
            pair,
            lanes,
            key,
            receptance,
            value,
            lat_ref,
            draise_ref,
            dbias_ref,
            rraise_ref,
            rbias_ref,
            tempo_ref,
            extra_ref,
            query_ref,
            local_ref,
            transfer_ref,
            carried_ref,
        ),
    )
    for load in loads[6:]:
        load.wait()
    edge[0] = pool_ref[:HALO]
    edge[1] = pool_ref[tokens - HALO :]

    sides = [(has_prev, prev, has_next), (has_next, after, has_prev)]
    def state_copy(d, p):
        return remote(
            leaving.at[d, p],
            incoming.at[d, p],
            ss.at[d, p],
            sr.at[d, p],
            "sp",
            after if d == 0 else prev,
        )

    halo_copies = [
        remote(edge.at[1], halo.at[0], hs.at[0], hr.at[0], "sp", after),
        remote(edge.at[0], halo.at[1], hs.at[1], hr.at[1], "sp", prev),
    ]
    sends = [has_next, has_prev]
    takes = [has_prev, has_next]

    def relay(d):
        @pl.when(jnp.logical_not(takes[d]))
        def _():
            incoming[d] = jnp.zeros_like(incoming[d])

        for p in range(pairs):

            @pl.when(takes[d])
            def _():
                state_copy(d, p).wait_recv()

            @pl.when(sends[d])
            def _():
                leaving[d, p] = (
                    dot(incoming[d, p], transfer_ref[d, p]) + carried_ref[d, p]
                ).astype(bf16)
                state_copy(d, p).start()

    def start_halo(d):
        pl.when(sends[d])(lambda: halo_copies[d].start())

    early = 2 * z < nsp

    @pl.when(early)
    def _():
        relay(0)

    @pl.when(jnp.logical_not(early))
    def _():
        relay(1)

    for d in range(2):
        start_halo(d)
    for d in range(2):

        @pl.when(takes[d])
        def _():
            halo_copies[d].wait_recv()

        @pl.when(jnp.logical_not(takes[d]))
        def _():
            halo[d] = jnp.zeros_like(halo[d])

    span = tokens + 2 * HALO
    rim = jnp.concatenate([halo[0], pool_ref[...], halo[1]], 0)
    here = lax.broadcasted_iota(jnp.int32, (tokens, span), 0)
    there = lax.broadcasted_iota(jnp.int32, (tokens, span), 1) - HALO
    position = z * tokens + lax.broadcasted_iota(jnp.int32, (tokens, GROUP_WIDTH), 0)
    length = tokens * nsp
    groups_here = channels // GROUP_WIDTH
    for member in range(groups_here):
        cols = slice(member * GROUP_WIDTH, (member + 1) * GROUP_WIDTH)
        reach = jnp.left_shift(1, core * groups_here + member)
        window = jnp.where((there >= here - reach) & (there < here + reach), 1.0, 0.0)
        total = dot(window, rim[:, cols])
        size = (
            jnp.minimum(position + reach, length) - jnp.maximum(position - reach, 0)
        ).astype(f32)
        diff = (total / size - pool_ref[:, cols].astype(f32)).astype(bf16)
        act[me, 0, :, cols] = dot(diff, mix_ref[member]).astype(bf16)
    order = list(range(nfs - 1, 0, -1))
    shares = []
    for d in order:
        peer = flipped(me, d)
        copy = remote(act.at[me, 0], act.at[me, 0], gs.at[d, 0], gr.at[d, 0], "fs", peer)
        copy.start()
        shares.append(copy)

    @pl.when(early)
    def _():
        relay(1)

    @pl.when(jnp.logical_not(early))
    def _():
        relay(0)

    head0 = lax.broadcasted_iota(jnp.int32, (tokens, LANES), 1) < HEAD
    top0 = lax.broadcasted_iota(jnp.int32, (HEAD, LANES), 1) < HEAD
    for p in range(pairs):
        lanes = slice(p * LANES, (p + 1) * LANES)
        readout = local_ref[:, lanes]
        for d in range(2):
            state = incoming[d, p].astype(f32)
            wide = jnp.concatenate(
                [jnp.where(top0, state, 0.0), jnp.where(top0, 0.0, state)], 0
            )
            readout = readout + dot_rows(query_ref[d, :, lanes], wide)

        def head_mean(cells):
            low = jnp.sum(jnp.where(head0, cells, 0.0), axis=-1, keepdims=True)
            high = jnp.sum(jnp.where(head0, 0.0, cells), axis=-1, keepdims=True)
            return jnp.where(head0, low, high) * (1.0 / HEAD)

        centred = readout - head_mean(readout)
        scaled = centred * lax.rsqrt(head_mean(centred * centred) + head_eps)
        act[me, 1, :, lanes] = (scaled * gain_ref[lanes].astype(f32).reshape(1, -1)).astype(bf16)
        if (p + 1) % (pairs // 2) == 0:
            part = (p + 1) // (pairs // 2)
            cols = pl.ds((part - 1) * (channels // 2), channels // 2)
            for d in order:
                copy = remote(
                    act.at[me, 1, :, cols],
                    act.at[me, 1, :, cols],
                    gs.at[d, part],
                    gr.at[d, part],
                    "fs",
                    flipped(me, d),
                )
                copy.start()
                shares.append(copy)

    other = lax.rem(core + 1, ntp)
    mine_at = pl.multiple_of(core * half_rows, half_rows)
    other_at = pl.multiple_of(other * half_rows, half_rows)

    def product(seq, rows):
        return dot_rows(act[seq, 1, rows], wa_ref[...]) + dot_rows(act[seq, 0, rows], wp_ref[...])

    returns = []
    swaps = []
    turns = [0] + order
    for d in turns:
        seq = flipped(me, d)
        if d:
            for copy, at in zip(shares, order * 3):
                if at == d:
                    copy.wait_recv()
        tsend[d] = product(seq, pl.ds(other_at, half_rows)).astype(bf16)
        swap = remote(tsend.at[d], trecv.at[d], ts.at[d], tr.at[d], "tp", other)
        swap.start()
        swaps.append(swap)
        kept = product(seq, pl.ds(mine_at, half_rows))
        swap.wait_recv()
        whole = (kept + trecv[d].astype(f32)).astype(bf16)
        if d:
            osend[d] = whole
            copy = remote(osend.at[d], orecv.at[me], os.at[d], orr.at[d], "fs", seq)
            copy.start()
            returns.append(copy)
        else:
            orecv[me] = whole
    for copy in returns:
        copy.wait_recv()
    for j in range(nfs):
        out_ref[0, :, j * channels : (j + 1) * channels] = orecv[j]
    for copy in shares + swaps + returns:
        copy.wait_send()
    for d in range(2):

        @pl.when(sends[d])
        def _():
            for p in range(pairs):
                state_copy(d, p).wait_send()
            halo_copies[d].wait_send()


def shards(
    inputs,
    input_norm_gain,
    receptance_matrix,
    key_matrix,
    value_matrix,
    pooling_input_weight,
    decay_lower_matrix,
    decay_raise_matrix,
    decay_offset_bias,
    removal_lower_matrix,
    removal_raise_matrix,
    removal_rate_bias,
    tempo_scale,
    sudden_decay_extra,
    head_norm_gain,
    group_mixing_weight,
    attention_output_matrix,
    pooling_output_matrix,
):
    nsp, nfs, ntp = lax.axis_size("sp"), lax.axis_size("fs"), lax.axis_size("tp")
    _, tokens, features = inputs.shape
    depth, channels = key_matrix.shape
    pairs = channels // LANES
    dma = pltpu.SemaphoreType.DMA
    rank = decay_lower_matrix.shape[1]
    rank2 = decay_raise_matrix.shape[0] * decay_raise_matrix.shape[1]
    anywhere = pl.BlockSpec(memory_space=pl.ANY)
    half = (nfs, tokens // ntp, depth)
    return pl.pallas_call(
        functools.partial(layer_kernel, nsp, nfs, ntp),
        out_shape=jax.ShapeDtypeStruct((1, tokens // ntp, features), bf16),
        in_specs=[VMEM] * 2
        + [anywhere] * 6
        + [VMEM] * 6
        + [anywhere, VMEM, anywhere, anywhere],
        out_specs=VMEM,
        scratch_shapes=[pltpu.VMEM((depth, channels), bf16)] * 4
        + [
            pltpu.VMEM((features, rank), bf16),
            pltpu.VMEM((features, rank), bf16),
            pltpu.VMEM(group_mixing_weight.shape, bf16),
            pltpu.VMEM(attention_output_matrix.shape, bf16),
            pltpu.VMEM(pooling_output_matrix.shape, bf16),
            dma((9,)),
            pltpu.VMEM((nfs, tokens, depth), bf16),
            pltpu.VMEM((nfs, tokens, depth), bf16),
            pltpu.VMEM((nfs, pairs, 3, tokens, LANES), bf16),
            pltpu.VMEM((nfs, tokens, channels), bf16),
            pltpu.VMEM((nfs, pairs, 3, tokens, LANES), bf16),
            pltpu.VMEM((nfs, tokens, channels), bf16),
            dma((nfs, ntp)),
            dma((nfs, ntp)),
            dma((nfs, pairs + 1)),
            dma((nfs, pairs + 1)),
            pltpu.VMEM((2, tokens, rank), bf16),
            pltpu.VMEM((tokens, channels), bf16),
            pltpu.VMEM((2, tokens, channels), bf16),
            pltpu.VMEM((tokens, channels), f32),
            pltpu.VMEM((2, pairs, LANES, LANES), f32),
            pltpu.VMEM((2, pairs, HEAD, LANES), f32),
            pltpu.VMEM((2, HALO, channels), bf16),
            pltpu.VMEM((2, HALO, channels), bf16),
            pltpu.VMEM((2, pairs, HEAD, LANES), bf16),
            pltpu.VMEM((2, pairs, HEAD, LANES), bf16),
            pltpu.VMEM((nfs, 2, tokens, channels), bf16),
            pltpu.VMEM(half, bf16),
            pltpu.VMEM(half, bf16),
            pltpu.VMEM(half, bf16),
            pltpu.VMEM(half, bf16),
            dma((2,)),
            dma((2,)),
            dma((2, pairs)),
            dma((2, pairs)),
            dma((nfs, 3)),
            dma((nfs, 3)),
            dma((nfs,)),
            dma((nfs,)),
            dma((nfs,)),
            dma((nfs,)),
        ],
        compiler_params=pltpu.CompilerParams(
            collective_id=0, has_side_effects=True, vmem_limit_bytes=60 * 1024 * 1024
        ),
        name="layer",
    )(
        inputs,
        input_norm_gain,
        key_matrix,
        receptance_matrix,
        value_matrix,
        pooling_input_weight,
        decay_lower_matrix,
        removal_lower_matrix,
        decay_raise_matrix.reshape(rank2, channels),
        decay_offset_bias,
        removal_raise_matrix.reshape(rank2, channels),
        removal_rate_bias,
        tempo_scale[0],
        sudden_decay_extra[0],
        group_mixing_weight,
        head_norm_gain,
        attention_output_matrix,
        pooling_output_matrix,
    )


def solution(mesh):
    in_specs = (
        P("fs", "sp", None),
        P(),
        P("fs", "tp"),
        P("fs", "tp"),
        P("fs", "tp"),
        P("fs", "tp"),
        P(),
        P(None, None, "tp"),
        P(None, "tp"),
        P(),
        P(None, None, "tp"),
        P(None, "tp"),
        P("fs", None, "tp", "sp"),
        P("fs", None, "tp", "sp"),
        P("tp"),
        P("tp", None, None),
        P("fs", "tp"),
        P("fs", "tp"),
    )
    out_specs = P("fs", ("sp", "tp"), None)
    return jax.shard_map(shards, mesh=mesh, in_specs=in_specs, out_specs=out_specs, check_vma=False)
```

```python
import functools

import jax
import jax.numpy as jnp
from jax import lax
from jax.experimental import pallas as pl
from jax.experimental.pallas import tpu as pltpu
from jax.sharding import PartitionSpec as P

HEAD = 64
GROUP_WIDTH = 256
LANES = 128
BLOCK = 16
HALO = 16

norm_eps = 1e-06
head_eps = 0.00064
unit_eps = 1e-06
f32 = jnp.float32
bf16 = jnp.bfloat16
VMEM = pl.BlockSpec(memory_space=pltpu.VMEM)


def dot(left, right):
    return jnp.dot(left.astype(bf16), right.astype(bf16), preferred_element_type=f32)


def dot_general(left, right, dims):
    return lax.dot_general(
        left.astype(bf16), right.astype(bf16), (dims, ((), ())), preferred_element_type=f32
    )


def dot_rows(left, right):
    return dot_general(left, right, ((1,), (1,)))


def dot_cols(left, right):
    return dot_general(left, right, ((0,), (0,)))


def pieces(cells):
    high = cells.astype(bf16).astype(f32)
    rest = cells - high
    middle = rest.astype(bf16).astype(f32)
    return jnp.concatenate([high, middle, rest - middle], 0)


def remote(src, dst, send, recv, axis, peer):
    return pltpu.make_async_remote_copy(
        src_ref=src,
        dst_ref=dst,
        send_sem=send,
        recv_sem=recv,
        device_id={axis: peer},
        device_id_type=pl.DeviceIdType.MESH,
    )


def greet(barrier, axis, peer):
    pl.semaphore_signal(
        barrier, inc=1, device_id={axis: peer}, device_id_type=pl.DeviceIdType.MESH
    )


def flipped(at, bits):
    moved = at
    bit = 1
    while bit <= bits:
        if bits & bit:
            moved = moved + bit - 2 * bit * lax.rem(at // bit, 2)
        bit *= 2
    return moved


def front_part(
    n,
    x_ref,
    gain_ref,
    weights,
    lowers,
    loads,
    pool_ref,
    lat_ref,
    mine,
    cells,
    part,
    pool_part,
    landed,
    pool_landed,
    xs,
    xr,
    ps,
    pr,
    count,
    mix_pair,
):
    me = lax.axis_index("fs")
    core, ntp = lax.axis_index("tp"), lax.axis_size("tp")
    width = x_ref.shape[2] // n
    share = x_ref.shape[1] // ntp
    rows = pl.ds(pl.multiple_of(core * share, share), share)
    pairs = part.shape[1]
    x = x_ref[0].astype(f32)
    normed = (
        x
        * lax.rsqrt(jnp.mean(x * x, axis=-1, keepdims=True) + norm_eps)
        * gain_ref[...].astype(f32).reshape(1, -1)
    ).astype(bf16)
    for j in range(n):
        mine[j] = normed[:, j * width : (j + 1) * width]
    pl.semaphore_wait(pltpu.get_barrier_semaphore(), count)
    order = list(range(n - 1, 0, -1))
    moves = []
    for d in order:
        peer = flipped(me, d)
        copy = remote(
            mine.at[peer, rows], cells.at[me, rows], xs.at[d, 0], xr.at[d, 0], "fs", peer
        )
        copy.start()
        moves.append(copy)
    for load in loads[:2]:
        load.wait()
    dl_ref, rl_ref = lowers
    decay = jnp.zeros((x.shape[0], dl_ref.shape[1]), f32)
    rate = jnp.zeros((x.shape[0], rl_ref.shape[1]), f32)
    for j in range(n):
        block = mine[j]
        decay = decay + dot(block, dl_ref[j * width : (j + 1) * width])
        rate = rate + dot(block, rl_ref[j * width : (j + 1) * width])
    lat_ref[0] = jnp.tanh(decay.astype(bf16).astype(f32)).astype(bf16)
    lat_ref[1] = rate.astype(bf16)
    for load in loads[2:]:
        load.wait()
    for d, copy in zip(order, list(moves)):
        peer = flipped(me, d)
        copy.wait_recv()
        for e in range(1, ntp):
            passed = remote(
                cells.at[peer, rows],
                cells.at[peer, rows],
                xs.at[d, e],
                xr.at[d, e],
                "tp",
                lax.rem(core + e, ntp),
            )
            passed.start()
            moves.append(passed)
    for copy in moves[len(order) :]:
        copy.wait_recv()

    def pair_copy(d, p):
        peer = flipped(me, d)
        return remote(
            part.at[peer, p], landed.at[me, p], ps.at[d, p], pr.at[d, p], "fs", peer
        )

    def pool_copy(d):
        peer = flipped(me, d)
        return remote(
            pool_part.at[peer],
            pool_landed.at[me],
            ps.at[d, pairs],
            pr.at[d, pairs],
            "fs",
            peer,
        )

    for p in range(pairs):
        for d in order:
            peer = flipped(me, d)
            for m in range(3):
                part[peer, p, m] = dot(
                    cells[peer], weights[m][:, p * LANES : (p + 1) * LANES]
                ).astype(bf16)
            pair_copy(d, p).start()
    for d in order:
        peer = flipped(me, d)
        pool_part[peer] = dot(cells[peer], weights[3][...]).astype(bf16)
        pool_copy(d).start()

    def pair_step(p, carry):
        lanes = pl.ds(pl.multiple_of(p * LANES, LANES), LANES)
        owned = [dot(mine[me], weights[m][:, lanes]) for m in range(3)]
        for d in range(1, n):
            pair_copy(d, p).wait_recv()
        for d in range(1, n):
            peer = flipped(me, d)
            owned = [o + landed[peer, p, m].astype(f32) for m, o in enumerate(owned)]
        mix_pair(p, lanes, *[o.astype(bf16) for o in owned])
        return carry

    lax.fori_loop(0, pairs, pair_step, 0)
    total = dot(mine[me], weights[3][...])
    for d in range(1, n):
        pool_copy(d).wait_recv()
    for d in range(1, n):
        total = total + pool_landed[flipped(me, d)].astype(f32)
    pool_ref[...] = total.astype(bf16)
    for copy in moves:
        copy.wait_send()
    for d in range(1, n):
        for p in range(pairs):
            pair_copy(d, p).wait_send()
        pool_copy(d).wait_send()


def mix_pair(
    pair,
    lanes,
    key,
    receptance,
    value,
    lat_ref,
    draise_ref,
    dbias_ref,
    rraise_ref,
    rbias_ref,
    tempo_ref,
    extra_ref,
    query_ref,
    local_ref,
    transfer_ref,
    carried_ref,
):
    tokens = key.shape[0]
    kf = key.astype(f32)
    rf = receptance.astype(f32)
    lane = lax.broadcasted_iota(jnp.int32, (tokens, LANES), 1)
    row = lax.broadcasted_iota(jnp.int32, (tokens, LANES), 0)
    head0 = lane < HEAD
    k2 = kf * kf
    s0 = jnp.sum(jnp.where(head0, k2, 0.0), axis=-1, keepdims=True)
    s1 = jnp.sum(jnp.where(head0, 0.0, k2), axis=-1, keepdims=True)
    unit = kf * lax.rsqrt(jnp.where(head0, s0, s1) + unit_eps)
    heads = tempo_ref.shape[1]
    spread = (
        lax.broadcasted_iota(jnp.int32, (heads, LANES), 0)
        == 2 * pair + lax.broadcasted_iota(jnp.int32, (heads, LANES), 1) // HEAD
    ).astype(f32)
    spread = jnp.concatenate([spread, spread, spread], 0)
    blocks = tokens // BLOCK
    zero_row = jnp.zeros((1, LANES), f32)
    eye = (row == lane).astype(f32)
    sizes = []
    size = 1
    while size < tokens:
        sizes.append(size)
        size *= 2

    def level_mask(k):
        return ((row >> (k + 1)) == (lane >> (k + 1))) & ((row >> k) != (lane >> k))

    ways = []
    for d in range(2):
        lat_mask = head0 if d == 0 else ~head0
        lat_d = jnp.where(lat_mask, lat_ref[0].astype(f32), 0.0)
        lat_r = jnp.where(lat_mask, lat_ref[1].astype(f32), 0.0)
        pre = dbias_ref[d : d + 1, lanes] + dot(lat_d, draise_ref[:, lanes])
        velocity = jax.nn.sigmoid(pre) * 0.6065306597126334
        tempo = dot_cols(pieces(tempo_ref[d]), spread)
        extra = dot_cols(pieces(extra_ref[d]), spread)
        ld = -velocity * tempo + extra
        rate = jax.nn.sigmoid(rbias_ref[d : d + 1, lanes] + dot(lat_r, rraise_ref[:, lanes]))
        removal = unit * rate
        written = kf * rate
        upto = (lane <= row) if d == 0 else (lane >= row)
        ones = upto.astype(f32)
        inner = dot(jnp.concatenate([ones, ones, ones], 1), pieces(ld))
        excl = inner - ld
        grams = []
        for i in range(blocks):
            lo, hi = i * BLOCK, (i + 1) * BLOCK
            if d == 0:
                base = inner[lo - 1 : lo] if i > 0 else zero_row
            else:
                base = inner[hi : hi + 1] if i < blocks - 1 else zero_row
            ahead = unit[lo:hi] * jnp.exp(excl[lo:hi] - base)
            query = rf[lo:hi] * jnp.exp(inner[lo:hi] - base)
            grow = jnp.exp(jnp.minimum(base - inner, 80.0))
            right = jnp.concatenate([(removal * grow).astype(bf16), (written * grow).astype(bf16)], 0)
            h0 = head0[lo:hi]
            left = jnp.concatenate(
                [
                    jnp.where(h0, ahead, 0.0),
                    jnp.where(h0, 0.0, ahead),
                    jnp.where(h0, query, 0.0),
                    jnp.where(h0, 0.0, query),
                ],
                0,
            )
            grams.append(dot_rows(left, right))
        strict = (lane < row) if d == 0 else (lane > row)

        def gathered(place, at, mask):
            rows = jnp.concatenate(
                [g[place * BLOCK : (place + 1) * BLOCK, at * tokens : (at + 1) * tokens] for g in grams],
                0,
            )
            return jnp.where(mask, rows, 0.0)

        way = dict(inner=inner, excl=excl, removal=removal, written=written)
        way["link"] = [gathered(h, 0, strict) for h in range(2)]
        way["link_write"] = [gathered(h, 1, strict).astype(bf16) for h in range(2)]
        way["read"] = [gathered(2 + h, 0, upto).astype(bf16) for h in range(2)]
        way["read_write"] = [gathered(2 + h, 1, upto).astype(bf16) for h in range(2)]
        ways.append(way)

    links = [way["link"][h] for way in ways for h in range(2)]
    inverses = [eye - jnp.where(level_mask(0), a, 0.0) for a in links]
    for k in range(1, len(sizes)):
        mask = level_mask(k)
        firsts = [dot(t, jnp.where(mask, a, 0.0)) for t, a in zip(inverses, links)]
        inverses = [t - dot(u, t) for t, u in zip(inverses, firsts)]

    block_diag = (row < HEAD) == head0
    local = jnp.zeros((tokens, LANES), f32)
    for d, way in enumerate(ways):
        inner, excl = way["inner"], way["excl"]
        last = inner[tokens - 1 : tokens] if d == 0 else inner[0:1]
        ahead = unit * jnp.exp(excl)
        query = rf * jnp.exp(inner)
        tail = jnp.exp(last - inner)

        def chosen(pieces):
            return jnp.where(head0, pieces[0], pieces[1])

        base = chosen([dot(way["link_write"][h], value) for h in range(2)])
        rhs = jnp.concatenate([ahead.astype(bf16), base.astype(bf16)], 1)
        solved = [dot(inverses[2 * d + h], rhs) for h in range(2)]
        pull_map = -chosen([s[:, :LANES] for s in solved])
        pull_base = -chosen([s[:, LANES:] for s in solved])
        remove_tail = (way["removal"] * tail).astype(bf16)
        write_tail = (way["written"] * tail).astype(bf16)
        both = jnp.concatenate([pull_map.astype(bf16), pull_base.astype(bf16)], 1)
        seen = [dot(way["read"][h], both) for h in range(2)]
        query_ref[d, :, lanes] = (query + chosen([s[:, :LANES] for s in seen])).astype(bf16)
        local = (
            local
            + chosen([s[:, LANES:] for s in seen])
            + chosen([dot(way["read_write"][h], value) for h in range(2)])
        )
        transfer = jnp.where(block_diag, dot_cols(pull_map, remove_tail), 0.0) + eye * jnp.exp(last)
        transfer_ref[d, pair] = transfer
        carried = dot_cols(
            jnp.concatenate([pull_base.astype(bf16), value], 0),
            jnp.concatenate([remove_tail, write_tail], 0),
        )
        carried = jnp.where(block_diag, carried, 0.0)
        carried_ref[d, pair] = carried[:HEAD] + carried[HEAD:]
    local_ref[:, lanes] = local


def layer_kernel(
    nsp,
    nfs,
    ntp,
    x_ref,
    in_gain_ref,
    wk_hbm,
    wr_hbm,
    wv_hbm,
    wi_hbm,
    dl_hbm,
    rl_hbm,
    draise_ref,
    dbias_ref,
    rraise_ref,
    rbias_ref,
    tempo_ref,
    extra_ref,
    mix_hbm,
    gain_ref,
    wa_hbm,
    wp_hbm,
    out_ref,
    wk_ref,
    wr_ref,
    wv_ref,
    wi_ref,
    dl_ref,
    rl_ref,
    mix_ref,
    wa_ref,
    wp_ref,
    loaded,
    mine,
    cells,
    part,
    pool_part,
    landed,
    pool_landed,
    xs,
    xr,
    ps,
    pr,
    lat_ref,
    pool_ref,
    query_ref,
    local_ref,
    transfer_ref,
    carried_ref,
    edge,
    halo,
    incoming,
    leaving,
    act,
    tsend,
    trecv,
    osend,
    orecv,
    hs,
    hr,
    ss,
    sr,
    gs,
    gr,
    ts,
    tr,
    os,
    orr,
):
    z = lax.axis_index("sp")
    me = lax.axis_index("fs")
    core = lax.axis_index("tp")
    tokens, channels = local_ref.shape
    pairs = transfer_ref.shape[1]
    half_rows = tokens // ntp
    has_prev = z > 0
    has_next = z < nsp - 1
    prev = jnp.maximum(z - 1, 0)
    after = jnp.minimum(z + 1, nsp - 1)

    barrier = pltpu.get_barrier_semaphore()
    for d in range(1, nfs):
        greet(barrier, "fs", flipped(me, d))
    for d in range(1, ntp):
        greet(barrier, "tp", lax.rem(core + d, ntp))
    pl.when(has_prev)(lambda: greet(barrier, "sp", prev))
    pl.when(has_next)(lambda: greet(barrier, "sp", after))
    count = nfs + ntp - 2 + jnp.where(has_prev, 1, 0) + jnp.where(has_next, 1, 0)
    sources = (dl_hbm, rl_hbm, wk_hbm, wr_hbm, wv_hbm, wi_hbm, mix_hbm, wa_hbm, wp_hbm)
    targets = (dl_ref, rl_ref, wk_ref, wr_ref, wv_ref, wi_ref, mix_ref, wa_ref, wp_ref)
    loads = [
        pltpu.make_async_copy(source, target, loaded.at[i])
        for i, (source, target) in enumerate(zip(sources, targets))
    ]
    for load in loads:
        load.start()
    front_part(
        nfs,
        x_ref,
        in_gain_ref,
        (wk_ref, wr_ref, wv_ref, wi_ref),
        (dl_ref, rl_ref),
        loads[:6],
        pool_ref,
        lat_ref,
        mine,
        cells,
        part,
        pool_part,
        landed,
        pool_landed,
        xs,
        xr,
        ps,
        pr,
        count,
        lambda pair, lanes, key, receptance, value: mix_pair(
            pair,
            lanes,
            key,
            receptance,
            value,
            lat_ref,
            draise_ref,
            dbias_ref,
            rraise_ref,
            rbias_ref,
            tempo_ref,
            extra_ref,
            query_ref,
            local_ref,
            transfer_ref,
            carried_ref,
        ),
    )
    for load in loads[6:]:
        load.wait()
    edge[0] = pool_ref[:HALO]
    edge[1] = pool_ref[tokens - HALO :]

    sides = [(has_prev, prev, has_next), (has_next, after, has_prev)]
    def state_copy(d, p):
        return remote(
            leaving.at[d, p],
            incoming.at[d, p],
            ss.at[d, p],
            sr.at[d, p],
            "sp",
            after if d == 0 else prev,
        )

    halo_copies = [
        remote(edge.at[1], halo.at[0], hs.at[0], hr.at[0], "sp", after),
        remote(edge.at[0], halo.at[1], hs.at[1], hr.at[1], "sp", prev),
    ]
    sends = [has_next, has_prev]
    takes = [has_prev, has_next]

    def relay(d):
        @pl.when(jnp.logical_not(takes[d]))
        def _():
            incoming[d] = jnp.zeros_like(incoming[d])

        for p in range(pairs):

            @pl.when(takes[d])
            def _():
                state_copy(d, p).wait_recv()

            @pl.when(sends[d])
            def _():
                leaving[d, p] = (
                    dot(incoming[d, p], transfer_ref[d, p]) + carried_ref[d, p]
                ).astype(bf16)
                state_copy(d, p).start()

    def start_halo(d):
        pl.when(sends[d])(lambda: halo_copies[d].start())

    early = 2 * z < nsp

    @pl.when(early)
    def _():
        relay(0)

    @pl.when(jnp.logical_not(early))
    def _():
        relay(1)

    for d in range(2):
        start_halo(d)
    for d in range(2):

        @pl.when(takes[d])
        def _():
            halo_copies[d].wait_recv()

        @pl.when(jnp.logical_not(takes[d]))
        def _():
            halo[d] = jnp.zeros_like(halo[d])

    span = tokens + 2 * HALO
    rim = jnp.concatenate([halo[0], pool_ref[...], halo[1]], 0)
    here = lax.broadcasted_iota(jnp.int32, (tokens, span), 0)
    there = lax.broadcasted_iota(jnp.int32, (tokens, span), 1) - HALO
    position = z * tokens + lax.broadcasted_iota(jnp.int32, (tokens, GROUP_WIDTH), 0)
    length = tokens * nsp
    groups_here = channels // GROUP_WIDTH
    for member in range(groups_here):
        cols = slice(member * GROUP_WIDTH, (member + 1) * GROUP_WIDTH)
        reach = jnp.left_shift(1, core * groups_here + member)
        window = jnp.where((there >= here - reach) & (there < here + reach), 1.0, 0.0)
        total = dot(window, rim[:, cols])
        size = (
            jnp.minimum(position + reach, length) - jnp.maximum(position - reach, 0)
        ).astype(f32)
        diff = (total / size - pool_ref[:, cols].astype(f32)).astype(bf16)
        act[me, 0, :, cols] = dot(diff, mix_ref[member]).astype(bf16)
    order = list(range(nfs - 1, 0, -1))
    shares = []
    for d in order:
        peer = flipped(me, d)
        copy = remote(act.at[me, 0], act.at[me, 0], gs.at[d, 0], gr.at[d, 0], "fs", peer)
        copy.start()
        shares.append(copy)

    @pl.when(early)
    def _():
        relay(1)

    @pl.when(jnp.logical_not(early))
    def _():
        relay(0)

    head0 = lax.broadcasted_iota(jnp.int32, (tokens, LANES), 1) < HEAD
    top0 = lax.broadcasted_iota(jnp.int32, (HEAD, LANES), 1) < HEAD
    for p in range(pairs):
        lanes = slice(p * LANES, (p + 1) * LANES)
        readout = local_ref[:, lanes]
        for d in range(2):
            state = incoming[d, p].astype(f32)
            wide = jnp.concatenate(
                [jnp.where(top0, state, 0.0), jnp.where(top0, 0.0, state)], 0
            )
            readout = readout + dot_rows(query_ref[d, :, lanes], wide)

        def head_mean(cells):
            low = jnp.sum(jnp.where(head0, cells, 0.0), axis=-1, keepdims=True)
            high = jnp.sum(jnp.where(head0, 0.0, cells), axis=-1, keepdims=True)
            return jnp.where(head0, low, high) * (1.0 / HEAD)

        centred = readout - head_mean(readout)
        scaled = centred * lax.rsqrt(head_mean(centred * centred) + head_eps)
        act[me, 1, :, lanes] = (scaled * gain_ref[lanes].astype(f32).reshape(1, -1)).astype(bf16)
        if (p + 1) % (pairs // 2) == 0:
            part = (p + 1) // (pairs // 2)
            cols = pl.ds((part - 1) * (channels // 2), channels // 2)
            for d in order:
                copy = remote(
                    act.at[me, 1, :, cols],
                    act.at[me, 1, :, cols],
                    gs.at[d, part],
                    gr.at[d, part],
                    "fs",
                    flipped(me, d),
                )
                copy.start()
                shares.append(copy)

    other = lax.rem(core + 1, ntp)
    mine_at = pl.multiple_of(core * half_rows, half_rows)
    other_at = pl.multiple_of(other * half_rows, half_rows)

    def product(seq, rows):
        return dot_rows(act[seq, 1, rows], wa_ref[...]) + dot_rows(act[seq, 0, rows], wp_ref[...])

    returns = []
    swaps = []
    turns = [0] + order
    for d in turns:
        seq = flipped(me, d)
        if d:
            for copy, at in zip(shares, order * 3):
                if at == d:
                    copy.wait_recv()
        tsend[d] = product(seq, pl.ds(other_at, half_rows)).astype(bf16)
        swap = remote(tsend.at[d], trecv.at[d], ts.at[d], tr.at[d], "tp", other)
        swap.start()
        swaps.append(swap)
        kept = product(seq, pl.ds(mine_at, half_rows))
        swap.wait_recv()
        whole = (kept + trecv[d].astype(f32)).astype(bf16)
        if d:
            osend[d] = whole
            copy = remote(osend.at[d], orecv.at[me], os.at[d], orr.at[d], "fs", seq)
            copy.start()
            returns.append(copy)
        else:
            orecv[me] = whole
    for copy in returns:
        copy.wait_recv()
    for j in range(nfs):
        out_ref[0, :, j * channels : (j + 1) * channels] = orecv[j]
    for copy in shares + swaps + returns:
        copy.wait_send()
    for d in range(2):

        @pl.when(sends[d])
        def _():
            for p in range(pairs):
                state_copy(d, p).wait_send()
            halo_copies[d].wait_send()


def shards(
    inputs,
    input_norm_gain,
    receptance_matrix,
    key_matrix,
    value_matrix,
    pooling_input_weight,
    decay_lower_matrix,
    decay_raise_matrix,
    decay_offset_bias,
    removal_lower_matrix,
    removal_raise_matrix,
    removal_rate_bias,
    tempo_scale,
    sudden_decay_extra,
    head_norm_gain,
    group_mixing_weight,
    attention_output_matrix,
    pooling_output_matrix,
):
    nsp, nfs, ntp = lax.axis_size("sp"), lax.axis_size("fs"), lax.axis_size("tp")
    _, tokens, features = inputs.shape
    depth, channels = key_matrix.shape
    pairs = channels // LANES
    dma = pltpu.SemaphoreType.DMA
    rank = decay_lower_matrix.shape[1]
    rank2 = decay_raise_matrix.shape[0] * decay_raise_matrix.shape[1]
    anywhere = pl.BlockSpec(memory_space=pl.ANY)
    half = (nfs, tokens // ntp, depth)
    return pl.pallas_call(
        functools.partial(layer_kernel, nsp, nfs, ntp),
        out_shape=jax.ShapeDtypeStruct((1, tokens // ntp, features), bf16),
        in_specs=[VMEM] * 2
        + [anywhere] * 6
        + [VMEM] * 6
        + [anywhere, VMEM, anywhere, anywhere],
        out_specs=VMEM,
        scratch_shapes=[pltpu.VMEM((depth, channels), bf16)] * 4
        + [
            pltpu.VMEM((features, rank), bf16),
            pltpu.VMEM((features, rank), bf16),
            pltpu.VMEM(group_mixing_weight.shape, bf16),
            pltpu.VMEM(attention_output_matrix.shape, bf16),
            pltpu.VMEM(pooling_output_matrix.shape, bf16),
            dma((9,)),
            pltpu.VMEM((nfs, tokens, depth), bf16),
            pltpu.VMEM((nfs, tokens, depth), bf16),
            pltpu.VMEM((nfs, pairs, 3, tokens, LANES), bf16),
            pltpu.VMEM((nfs, tokens, channels), bf16),
            pltpu.VMEM((nfs, pairs, 3, tokens, LANES), bf16),
            pltpu.VMEM((nfs, tokens, channels), bf16),
            dma((nfs, ntp)),
            dma((nfs, ntp)),
            dma((nfs, pairs + 1)),
            dma((nfs, pairs + 1)),
            pltpu.VMEM((2, tokens, rank), bf16),
            pltpu.VMEM((tokens, channels), bf16),
            pltpu.VMEM((2, tokens, channels), bf16),
            pltpu.VMEM((tokens, channels), f32),
            pltpu.VMEM((2, pairs, LANES, LANES), f32),
            pltpu.VMEM((2, pairs, HEAD, LANES), f32),
            pltpu.VMEM((2, HALO, channels), bf16),
            pltpu.VMEM((2, HALO, channels), bf16),
            pltpu.VMEM((2, pairs, HEAD, LANES), bf16),
            pltpu.VMEM((2, pairs, HEAD, LANES), bf16),
            pltpu.VMEM((nfs, 2, tokens, channels), bf16),
            pltpu.VMEM(half, bf16),
            pltpu.VMEM(half, bf16),
            pltpu.VMEM(half, bf16),
            pltpu.VMEM(half, bf16),
            dma((2,)),
            dma((2,)),
            dma((2, pairs)),
            dma((2, pairs)),
            dma((nfs, 3)),
            dma((nfs, 3)),
            dma((nfs,)),
            dma((nfs,)),
            dma((nfs,)),
            dma((nfs,)),
        ],
        compiler_params=pltpu.CompilerParams(
            collective_id=0, has_side_effects=True, vmem_limit_bytes=60 * 1024 * 1024
        ),
        name="layer",
    )(
        inputs,
        input_norm_gain,
        key_matrix,
        receptance_matrix,
        value_matrix,
        pooling_input_weight,
        decay_lower_matrix,
        removal_lower_matrix,
        decay_raise_matrix.reshape(rank2, channels),
        decay_offset_bias,
        removal_raise_matrix.reshape(rank2, channels),
        removal_rate_bias,
        tempo_scale[0],
        sudden_decay_extra[0],
        group_mixing_weight,
        head_norm_gain,
        attention_output_matrix,
        pooling_output_matrix,
    )


def solution(mesh):
    in_specs = (
        P("fs", "sp", None),
        P(),
        P("fs", "tp"),
        P("fs", "tp"),
        P("fs", "tp"),
        P("fs", "tp"),
        P(),
        P(None, None, "tp"),
        P(None, "tp"),
        P(),
        P(None, None, "tp"),
        P(None, "tp"),
        P("fs", None, "tp", "sp"),
        P("fs", None, "tp", "sp"),
        P("tp"),
        P("tp", None, None),
        P("fs", "tp"),
        P("fs", "tp"),
    )
    out_specs = P("fs", ("sp", "tp"), None)
    return jax.shard_map(shards, mesh=mesh, in_specs=in_specs, out_specs=out_specs, check_vma=False)
```
